512 devices in a mesh: sp: 64 (over z, y), tp: 8 (over x, core).
Axes of the slice: x: 4, y: 4, z: 16, core: 2. Of those that a mesh axis runs over, the one named last changes fastest.
Arguments:
- stream: bfloat16 [8192, 2048], P('sp'), may hold values from -6 to 6
- query_narrow: bfloat16 [8192, 512], P('sp', 'tp'), may hold values from -7 to 7
- query_broad: bfloat16 [8192, 1024], P('sp', 'tp'), may hold values from -7 to 7
- key_narrow: bfloat16 [8192, 512], P('sp', 'tp'), may hold values from -7 to 7
- key_broad: bfloat16 [8192, 1024], P('sp', 'tp'), may hold values from -7 to 7
- value_narrow: bfloat16 [8192, 512], P('sp', 'tp'), may hold values from -6 to 6
- value_broad: bfloat16 [8192, 1024], P('sp', 'tp'), may hold values from -6 to 6
- key_offsets: float32 [8192, 16], P('sp', 'tp'), may hold values from -20 to 0
- out_narrow: bfloat16 [512, 2048], P('tp'), may hold values from -0.4375 to 0.4375
- out_broad: bfloat16 [1024, 2048], P('tp'), may hold values from -0.4375 to 0.4375
- norm_gain: float32 [2048], replicated, may hold values from 0.1 to 1.9
- gate_weight: bfloat16 [2048, 3072], P('sp', 'tp'), may hold values from -0.125 to 0.125
- up_weight: bfloat16 [2048, 3072], P('sp', 'tp'), may hold values from -0.125 to 0.125
- down_weight: bfloat16 [3072, 2048], P('tp', 'sp'), may hold values from -0.21875 to 0.21875
Outputs:
- result: bfloat16 [8192, 2048], P(('sp', 'tp'))
The draws below stay inside these ranges and needn't reach their ends.
All inputs are finite; a program needn't handle non-finite values.
Results may differ from the reference program's by a relative error of at most 0.028.
Values may be sent and summed in bfloat16 or wider, within the bound.
A program may use at most 64 MiB of HBM per device.

```python
import jax
import jax.numpy as jnp
from jax import lax

D = 2048
FF = 3072
NARROW_HEADS = 8
NARROW_SIZE = 64
BROAD_HEADS = 8
BROAD_SIZE = 128
TOK_DEV = 128
SEQUENCE_TOKENS = 8192
N_TP = 8


def draw_key_offsets(key, part):
    parallel_flows = jax.random.split(jax.random.fold_in(key, 17), 6)
    column_indices = 2 * NARROW_HEADS
    fast_share = 0.5
    spread = 0.7
    fast = jax.random.uniform(parallel_flows[0], (column_indices,), jnp.float32) < fast_share
    slow_base = -2.0 - jnp.log(jnp.float32(SEQUENCE_TOKENS)) + jax.random.uniform(parallel_flows[1], (column_indices,), jnp.float32, -0.5, 0.5)
    base = jnp.where(fast, -3.5, slow_base)
    shifts = jax.random.uniform(parallel_flows[2], (SEQUENCE_TOKENS // TOK_DEV, 1, column_indices), jnp.float32, -spread, spread)
    moved_forward = (base[None, None, :] + shifts + jnp.zeros((SEQUENCE_TOKENS // TOK_DEV, TOK_DEV, column_indices), jnp.float32)).reshape(SEQUENCE_TOKENS, column_indices)
    coarse_estimate = jax.random.uniform(parallel_flows[3], (SEQUENCE_TOKENS, column_indices), jnp.float32, -0.5, 0.5)
    arrival_group = jax.random.uniform(parallel_flows[4], (SEQUENCE_TOKENS, column_indices), jnp.float32) < 4.0 / SEQUENCE_TOKENS
    arrival_value = jax.random.uniform(parallel_flows[5], (SEQUENCE_TOKENS, column_indices), jnp.float32, -2.5, -1.0)
    return jnp.where(arrival_group, arrival_value, moved_forward + coarse_estimate).astype(jnp.float32)


def steps_of(own_key, dims, shards, low, high):
    factor_of, own = 1.0, jax.random.fold_in(own_key, 6)
    for position, blocks in shards:
        steps = jnp.exp(jax.random.uniform(jax.random.fold_in(own, position), (blocks,), jnp.float32, low / len(shards), high / len(shards)))
        factor_of = factor_of * jnp.repeat(steps, dims[position] // blocks).reshape([-1 if axis == position else 1 for axis in range(len(dims))])
    return factor_of


def noise(key, extent, width, limit, cuts=(), kind=jnp.bfloat16):
    array = jax.random.normal(key, extent, jnp.float32) * width
    if len(cuts) > 0:
        array = steps_of(key, extent, cuts, -0.22, 0.18) * array
    return jnp.clip(array, min=-limit, max=limit).astype(kind)


def setup_inputs(seed: int = 0) -> dict:
    seeds = jax.random.split(jax.random.key(seed), 15)
    return {
        "stream": noise(seeds[0], (SEQUENCE_TOKENS, D), 1.0, 6.0, ((0, 64),)),
        "query_narrow": noise(seeds[1], (SEQUENCE_TOKENS, NARROW_HEADS * NARROW_SIZE), 1.2, 7.0, ((0, 64), (1, 8))),
        "query_broad": noise(seeds[2], (SEQUENCE_TOKENS, BROAD_HEADS * BROAD_SIZE), 1.2, 7.0, ((0, 64), (1, 8))),
        "key_narrow": noise(seeds[3], (SEQUENCE_TOKENS, NARROW_HEADS * NARROW_SIZE), 1.2, 7.0, ((0, 64), (1, 8))),
        "key_broad": noise(seeds[4], (SEQUENCE_TOKENS, BROAD_HEADS * BROAD_SIZE), 1.2, 7.0, ((0, 64), (1, 8))),
        "value_narrow": noise(seeds[5], (SEQUENCE_TOKENS, NARROW_HEADS * NARROW_SIZE), 1.0, 6.0, ((0, 64), (1, 8))),
        "value_broad": noise(seeds[6], (SEQUENCE_TOKENS, BROAD_HEADS * BROAD_SIZE), 1.0, 6.0, ((0, 64), (1, 8))),
        "key_offsets": draw_key_offsets(jax.random.fold_in(seeds[14], 71), 0),
        "out_narrow": noise(seeds[8], (NARROW_HEADS * NARROW_SIZE, D), ((NARROW_HEADS * NARROW_SIZE + BROAD_HEADS * BROAD_SIZE) // 9) ** -0.5, 0.4375, ((0, 8),)),
        "out_broad": noise(seeds[9], (BROAD_HEADS * BROAD_SIZE, D), ((NARROW_HEADS * NARROW_SIZE + BROAD_HEADS * BROAD_SIZE) // 9) ** -0.5, 0.4375, ((0, 8),)),
        "norm_gain": jnp.clip(1.0 + 0.18 * jax.random.normal(seeds[10], (D,), jnp.float32), 0.1, 1.9),
        "gate_weight": noise(seeds[11], (D, FF), D ** -0.5, 0.125, ((0, 64), (1, 8))),
        "up_weight": noise(seeds[12], (D, FF), D ** -0.5, 0.125, ((0, 64), (1, 8))),
        "down_weight": noise(seeds[13], (FF, D), (FF // 4) ** -0.5, 0.21875, ((0, 8), (1, 64))),
    }


def stick_heads(query, keys, values, offsets, heads, size):
    total = query.shape[0]
    qblock = 512 if total % 512 == 0 else total
    scale = size ** (-0.5)
    pieces = []
    for head in range(heads):
        query_head = query[:, head * size:(head + 1) * size]
        key_head = keys[:, head * size:(head + 1) * size]
        value_head = values[:, head * size:(head + 1) * size]
        offset_head = offsets[:, head]

        def one_block(index):
            first = (index * qblock).astype(jnp.int32)
            rows_q = lax.dynamic_slice_in_dim(query_head, first, qblock, 0)
            logits = jnp.dot(rows_q, jnp.transpose(key_head), preferred_element_type=jnp.float32) * scale + offset_head[None, :]
            tpos = first + jnp.arange(qblock, dtype=jnp.int32)
            spos = jnp.arange(total, dtype=jnp.int32)
            causal = spos[None, :] < tpos[:, None]
            lognot = jnp.where(causal, jax.nn.log_sigmoid(-logits), 0.0)
            later = lax.cumsum(lognot, axis=1, reverse=True) - lognot
            weights = jnp.where(causal, jnp.exp(jax.nn.log_sigmoid(logits) + later), 0.0).astype(jnp.bfloat16)
            return jnp.dot(weights, value_head, preferred_element_type=jnp.float32)
        blocks = lax.map(one_block, jnp.arange(total // qblock, dtype=jnp.int32))
        pieces.append(blocks.reshape(total, size).astype(jnp.bfloat16))
    return jnp.concatenate(pieces, axis=1)

def rounded(value):
    return lax.optimization_barrier(value.astype(jnp.bfloat16)).astype(jnp.float32)

def reference(stream, query_narrow, query_broad, key_narrow, key_broad, value_narrow, value_broad, key_offsets, out_narrow, out_broad, norm_gain, gate_weight, up_weight, down_weight):
    attended_narrow = stick_heads(query_narrow, key_narrow, value_narrow, key_offsets[:, 0::2], NARROW_HEADS, NARROW_SIZE)
    attended_broad = stick_heads(query_broad, key_broad, value_broad, key_offsets[:, 1::2], BROAD_HEADS, BROAD_SIZE)
    width_narrow = NARROW_HEADS // N_TP * NARROW_SIZE
    width_broad = BROAD_HEADS // N_TP * BROAD_SIZE
    total = jnp.zeros((stream.shape[0], D), jnp.float32)
    for index in range(N_TP):
        part = jnp.dot(attended_narrow[:, index * width_narrow:(index + 1) * width_narrow], out_narrow[index * width_narrow:(index + 1) * width_narrow], preferred_element_type=jnp.float32)
        part = part + jnp.dot(attended_broad[:, index * width_broad:(index + 1) * width_broad], out_broad[index * width_broad:(index + 1) * width_broad], preferred_element_type=jnp.float32)
        total = total + rounded(part)
    mid = (stream.astype(jnp.float32) + total).astype(jnp.bfloat16)
    middle = mid.astype(jnp.float32)
    normed = (middle * lax.rsqrt(lax.optimization_barrier(jnp.mean(middle * middle, axis=1, keepdims=True)) + 1e-06) * norm_gain).astype(jnp.bfloat16)
    gate = jnp.dot(normed, gate_weight, preferred_element_type=jnp.float32)
    up = jnp.dot(normed, up_weight, preferred_element_type=jnp.float32)
    hidden = (jax.nn.silu(gate) * up).astype(jnp.bfloat16)
    hidden_width = FF // N_TP
    mixed = jnp.zeros((stream.shape[0], D), jnp.float32)
    for index in range(N_TP):
        part = jnp.dot(hidden[:, index * hidden_width:(index + 1) * hidden_width], down_weight[index * hidden_width:(index + 1) * hidden_width], preferred_element_type=jnp.float32)
        mixed = mixed + rounded(part)
    return (middle + mixed).astype(jnp.bfloat16)
```

```python
import functools
import math

import jax
import jax.numpy as jnp
from jax import lax
from jax.experimental import pallas as pl
from jax.experimental.pallas import tpu as pltpu
from jax.sharding import Mesh
from jax.sharding import PartitionSpec as P

NARROW_SIZE = 64
BROAD_SIZE = 128
SP = ("sp_0", "sp_1")
SP_TP = ("sp_0", "sp_1", "tp")
MESH = pl.DeviceIdType.MESH
LOG2E = 1.4426950408889634
SCALE = (NARROW_SIZE**-0.5 * LOG2E, BROAD_SIZE**-0.5 * LOG2E)
norm_eps = 1e-06
F32 = jnp.float32
BF16 = jnp.bfloat16
NT = (((1,), (1,)), ((), ()))
NN = (((1,), (0,)), ((), ()))


def dot(a, b, dims=NN, precision=None):
    return lax.dot_general(a, b, dims, preferred_element_type=F32, precision=precision)


def wrap(value, size):
    return lax.rem(value + 2 * size, size)


def layer_kernel(
    nz, ny, nt, rows, wrows, share,
    kv_in, off_in, q_in, gu_in, dt_in, stream_in, on_in, ob_in, gain_in,
    out,
    kv, off, qs, w, db, ow, st, gain, obuf, tall, ar, ao, part, rs, nb, mid_s, part2, rs2, hid,
    lsem, kvs, kvr, offs, offr, ws, wr, ds_, dr, q_s, q_r, dts, dtr, yas, yar, yrs, yrr,
    t_s, t_r, a_s, a_r, r1s, r1r, n_s, n_r, r2s, r2r,
):
    z = lax.axis_index("sp_0")
    y = lax.axis_index("sp_1")
    t = lax.axis_index("tp")
    up = (wrap(z + 1, nz), y, t)
    dn = (wrap(z - 1, nz), y, t)
    yp = (z, wrap(y + 1, ny), t)
    ym = (z, wrap(y - 1, ny), t)
    half = nz // 2

    def ypeer(j):
        return (z, wrap(y + j, ny), t)

    def tpeer(j):
        return (z, y, wrap(t + j, nt))

    def rc(src, dst, ssem, rsem, dev):
        return pltpu.make_async_remote_copy(
            src_ref=src, dst_ref=dst, send_sem=ssem, recv_sem=rsem,
            device_id=dev, device_id_type=MESH,
        )

    first = [
        pltpu.make_async_copy(kv_in, kv.at[z], lsem.at[0]),
        pltpu.make_async_copy(off_in, off.at[z], lsem.at[1]),
        pltpu.make_async_copy(q_in, qs.at[y], lsem.at[2]),
        pltpu.make_async_copy(gu_in, w.at[z, y], lsem.at[3]),
        pltpu.make_async_copy(dt_in, db.at[z, y], lsem.at[4]),
    ]
    second = [
        pltpu.make_async_copy(stream_in.at[pl.ds(t * share, share), :], st, lsem.at[5]),
        pltpu.make_async_copy(on_in, ow.at[pl.ds(64, 64), :], lsem.at[6]),
        pltpu.make_async_copy(ob_in, ow.at[pl.ds(128, 128), :], lsem.at[7]),
        pltpu.make_async_copy(gain_in, gain, lsem.at[8]),
    ]
    for c in first:
        c.start()
    for c in second:
        c.start()

    barrier = pltpu.get_barrier_semaphore()
    peers = [up, dn] + [ypeer(j) for j in range(1, ny)] + [tpeer(j) for j in range(1, nt)]
    for p in peers:
        pl.semaphore_signal(barrier, inc=1, device_id=p, device_id_type=MESH)

    ow[pl.ds(0, 64), :] = jnp.zeros((64, ow.shape[1]), BF16)
    tall[y] = jnp.zeros(tall.shape[1:], F32)

    def zero_body(i, carry):
        obuf[i] = jnp.zeros(obuf.shape[1:], F32)
        return carry

    lax.fori_loop(0, nz, zero_body, 0)
    for c in first:
        c.wait()
    pl.semaphore_wait(barrier, len(peers))

    def ring(buf, ssem, rsem, d, k, sub=None):
        zz = wrap(z - k + 1, nz) if d == 0 else wrap(z + k - 1, nz)
        ref = buf.at[zz] if sub is None else buf.at[zz, sub]
        return rc(ref, ref, ssem.at[d, k], rsem.at[d, k], up if d == 0 else dn)

    def kv_ring(d, k):
        return ring(kv, kvs, kvr, d, k)

    def off_ring(d, k):
        return ring(off, offs, offr, d, k)

    def w_ring(d, k):
        return ring(w, ws, wr, d, k, y)

    def d_ring(d, k):
        return ring(db, ds_, dr, d, k)

    def shard_z(d, k):
        return wrap(z - k, nz) if d == 0 else wrap(z + k, nz)

    def w_y(d, k, e):
        ref = w.at[shard_z(d, k), y]
        return rc(ref, ref, yas.at[d, k, e], yar.at[d, k, e], yp if e == 0 else ym)

    def w_relay(d, k):
        src_y = wrap(y - 1, ny) if d == 0 else wrap(y + 1, ny)
        ref = w.at[shard_z(d, k), src_y]
        return rc(ref, ref, yrs.at[d, k], yrr.at[d, k], yp if d == 0 else ym)

    def q_send(j):
        return rc(qs.at[y], qs.at[y], q_s.at[j], q_r.at[j], ypeer(j))

    def dt_send(j):
        return rc(db.at[z, y], db.at[z, y], dts.at[j], dtr.at[j], ypeer(j))

    def t_send(g, j):
        ref = tall.at[y, g]
        return rc(ref, ref, t_s.at[g, j], t_r.at[g, j], ypeer(j))

    for j in range(1, ny):
        q_send(j).start()
    for d in range(2):
        kv_ring(d, 1).start()
        off_ring(d, 1).start()
    for d in range(2):
        w_ring(d, 1).start()
    for j in range(1, ny):
        dt_send(j).start()
    for e in range(2):
        w_y(0, 0, e).start()

    key_row = lax.broadcasted_iota(jnp.int32, (rows, rows), 0)
    key_col = lax.broadcasted_iota(jnp.int32, (rows, rows), 1)
    tri = jnp.where(key_row > key_col, 1.0, 0.0).astype(BF16)
    sub_row = lax.broadcasted_iota(jnp.int32, (8, rows), 0)

    def process(zz, s, diag):
        def row_block(rb, carry):
            total = None
            for h in range(2):
                q = qs[rb, pl.ds(h * rows, rows), :]
                k = kv[zz, pl.ds(h * rows, rows), :]
                v = kv[zz, pl.ds(2 * h * rows, rows), :]
                logits = dot(q, k, NT) * SCALE[h] + off[zz, pl.ds(h, 1), :]
                soft = jnp.maximum(
                    jnp.log2(1.0 + jnp.exp2(jnp.minimum(logits, 126.0))), logits
                )
                if diag:
                    causal = (y * rows + key_col) < (rb * rows + key_row)
                    low = jnp.where(causal, soft, 0.0).astype(BF16)
                else:
                    low = soft.astype(BF16)
                after = dot(low, tri)
                weight = jnp.exp2(logits - soft - after)
                if diag:
                    weight = jnp.where(causal, weight, 0.0)
                obuf[s, h, pl.ds(rb * rows, rows), :] = dot(weight.astype(BF16), v)
                pick = jnp.where(sub_row == 2 * lax.rem(s, 4) + h, 1.0, 0.0).astype(BF16)
                mine = dot(pick, low, NT)
                total = mine if total is None else total + mine
            place = pl.ds(pl.multiple_of(rb * rows, rows), rows)
            g = lax.div(s, 4)
            tall[y, g, :, place] = tall[y, g, :, place] + total
            return carry

        lax.fori_loop(0, ny, row_block, 0)

    for j in range(1, ny):
        q_send(j).wait_recv()
    process(z, jnp.int32(0), True)

    def step(k, last):
        dirs = (0,) if last else (0, 1)
        for d in dirs:
            kv_ring(d, k).wait_recv()
            off_ring(d, k).wait_recv()
            if not last:
                if d == 0:
                    kv_ring(0, k + 1).start()
                    off_ring(0, k + 1).start()
                else:
                    @pl.when(k < half - 1)
                    def _():
                        kv_ring(1, k + 1).start()
                        off_ring(1, k + 1).start()
        for d in dirs:
            w_ring(d, k).wait_recv()
            if not last:
                if d == 0:
                    w_ring(0, k + 1).start()
                else:
                    @pl.when(k < half - 1)
                    def _():
                        w_ring(1, k + 1).start()
            for e in range(2):
                w_y(d, k, e).start()
        w_y(0, k - 1, 0).wait_recv()
        w_relay(0, k - 1).start()

        @pl.when(k >= 2)
        def _():
            w_y(1, k - 1, 1).wait_recv()
            w_relay(1, k - 1).start()

        @pl.when(k <= z)
        def _():
            process(wrap(z - k, nz), 2 * k - 1, False)

        if not last:
            @pl.when(z + k >= nz)
            def _():
                process(wrap(z + k, nz), 2 * k, False)

        @pl.when(lax.rem(k, 2) == 0)
        def _():
            for j in range(1, ny):
                t_send(lax.div(k, 2) - 1, j).start()

    def step_body(k, carry):
        step(k, False)
        return carry

    lax.fori_loop(1, half, step_body, 0)
    step(jnp.int32(half), True)

    for j in range(1, ny):
        dt_send(j).wait_recv()
    d_ring(0, 1).start()
    d_ring(1, 1).start()

    def d_step(k):
        if k > half:
            return
        d_ring(0, k).wait_recv()
        if k < half:
            d_ring(0, k + 1).start()
        if k < half:
            d_ring(1, k).wait_recv()
            if k < half - 1:
                d_ring(1, k + 1).start()

    w_y(0, half, 0).wait_recv()
    w_relay(0, half).start()

    ngroup = nz // 4
    for g in range(ngroup):
        for j in range(1, ny):
            t_send(g, j).wait_recv()
    d_step(1)

    trows = ny * ngroup * 8
    flat = tall[...].reshape(trows, ny * rows)
    fr = lax.broadcasted_iota(jnp.int32, (128, trows), 0)
    fc = lax.broadcasted_iota(jnp.int32, (128, trows), 1)

    def slot_z(slot):
        k = lax.shift_right_logical(slot + 1, 1)
        signed = jnp.where(lax.bitwise_and(slot, 1) == 1, -k, k)
        return lax.bitwise_and(z + signed + nz, nz - 1)

    per_y = ngroup * 8
    c_y = lax.div(fc, per_y)
    c_in = lax.rem(fc, per_y)
    r_order = slot_z(lax.shift_right_logical(fr, 1)) * ny + y
    c_order = slot_z(lax.shift_right_logical(c_in, 1)) * ny + c_y
    same = lax.bitwise_and(fr, 1) == lax.bitwise_and(c_in, 1)
    sel = jnp.where(jnp.logical_and(same, c_order > r_order), 1.0, 0.0).astype(F32)
    later = dot(sel, flat, NN, lax.Precision.HIGHEST)
    factor = jnp.exp2(-later)
    for rb in range(ny):
        ft = jnp.transpose(factor[:, rb * rows : (rb + 1) * rows])
        for h in range(2):
            acc = jnp.zeros((rows, 128), F32)
            for s in range(nz):
                col = lax.slice(ft, (0, 2 * s + h), (rows, 2 * s + h + 1))
                acc = acc + col * obuf[s, h, rb * rows : (rb + 1) * rows, :]
            ao[rb, :, h * 128 : (h + 1) * 128] = acc.astype(BF16)

    def a_send(j):
        peer = wrap(y + j, ny)
        return rc(ao.at[peer], ar.at[j], a_s.at[j], a_r.at[j], ypeer(j))

    for j in range(1, ny):
        a_send(j).start()
    d_step(2)
    d_step(3)
    for c in second:
        c.wait()
    attended = ao[y].astype(F32)
    for j in range(1, ny):
        a_send(j).wait_recv()
        attended = attended + ar[j].astype(F32)
    attended = attended.astype(BF16)
    model = out.shape[1]
    for c in range(model // 512):
        block = dot(attended, ow[:, c * 512 : (c + 1) * 512]).astype(BF16)
        part[:, :, c * 512 : (c + 1) * 512] = block.reshape(nt, share, 512)

    def r1_send(j):
        return rc(part.at[wrap(t + j, nt)], rs.at[j], r1s.at[j], r1r.at[j], tpeer(j))

    for j in range(1, nt):
        r1_send(j).start()
    d_step(4)
    d_step(5)
    total = st[...].astype(F32) + part[t].astype(F32)
    for j in range(1, nt):
        r1_send(j).wait_recv()
        total = total + rs[j].astype(F32)
    mid = total.astype(BF16).astype(F32)
    mid_s[...] = mid
    normed = mid * lax.rsqrt(jnp.mean(mid * mid, axis=1, keepdims=True) + norm_eps) * gain[...]
    nb[t] = normed.astype(BF16)

    def n_send(j):
        return rc(nb.at[t], nb.at[t], n_s.at[j], n_r.at[j], tpeer(j))

    for j in range(1, nt):
        n_send(j).start()
    for k in range(6, half + 1):
        d_step(k)

    def w_wait(k, d):
        if d == 0:
            w_y(0, k, 1).wait_recv()
            w_relay(0, k).wait_recv()
        else:
            w_y(1, k, 0).wait_recv()
            w_relay(1, k).wait_recv()

    def w_wait_body(k, carry):
        w_wait(k, 0)

        @pl.when(jnp.logical_and(k >= 1, k < half))
        def _():
            w_wait(k, 1)

        return carry

    lax.fori_loop(0, half + 1, w_wait_body, 0)
    for j in range(1, nt):
        n_send(j).wait_recv()

    gate = jnp.zeros((rows, w.shape[3]), F32)
    upv = jnp.zeros((rows, w.shape[3]), F32)
    span = ny * wrows
    for zz in range(nz):
        lhs = nb[:, :, zz * span : (zz + 1) * span].reshape(rows, span)
        gate = gate + dot(lhs, w[zz, :, 0:wrows, :].reshape(span, w.shape[3]))
        upv = upv + dot(lhs, w[zz, :, wrows : 2 * wrows, :].reshape(span, w.shape[3]))
    hidden = (gate / (1.0 + jnp.exp(-gate)) * upv).astype(BF16)
    for zz in range(nz):
        rhs = db[zz].reshape(span, db.shape[3])
        block = dot(hidden, rhs, NT).astype(BF16)
        part2[:, :, zz * span : (zz + 1) * span] = block.reshape(nt, share, span)

    def r2_send(j):
        return rc(part2.at[wrap(t + j, nt)], rs2.at[j], r2s.at[j], r2r.at[j], tpeer(j))

    for j in range(1, nt):
        r2_send(j).start()

    def drain(k, carry):
        for d in range(2):
            @pl.when(k <= half - d)
            def _():
                kv_ring(d, k).wait_send()
                off_ring(d, k).wait_send()
                w_ring(d, k).wait_send()
                d_ring(d, k).wait_send()
                for e in range(2):
                    w_y(d, k, e).wait_send()
                w_relay(d, k).wait_send()
        return carry

    lax.fori_loop(1, half + 1, drain, 0)
    for e in range(2):
        w_y(0, 0, e).wait_send()
    w_relay(0, 0).wait_send()
    for j in range(1, ny):
        q_send(j).wait_send()
        dt_send(j).wait_send()
        a_send(j).wait_send()
        for g in range(ngroup):
            t_send(g, j).wait_send()
    for j in range(1, nt):
        r1_send(j).wait_send()
        n_send(j).wait_send()
    total = mid_s[...] + part2[t].astype(F32)
    for j in range(1, nt):
        r2_send(j).wait_recv()
        total = total + rs2[j].astype(F32)
    out[...] = total.astype(BF16)
    for j in range(1, nt):
        r2_send(j).wait_send()


def local(
    nz, ny, nt,
    stream, query_narrow, query_broad, key_narrow, key_broad, value_narrow, value_broad,
    key_offsets, out_narrow, out_broad, norm_gain, gate_weight, up_weight, down_weight,
):
    rows, model = stream.shape
    wrows, ff = gate_weight.shape
    share = rows // nt
    half = nz // 2
    ngroup = nz // 4
    kv = jnp.concatenate(
        [jnp.concatenate([key_narrow, value_narrow], axis=1), key_broad, value_broad], axis=0
    )
    q = jnp.concatenate([jnp.pad(query_narrow, ((0, 0), (0, 64))), query_broad], axis=0)
    off = jnp.pad(jnp.transpose(key_offsets) * LOG2E, ((0, 6), (0, 0)))
    gu = jnp.concatenate([gate_weight, up_weight], axis=0)
    dt = jnp.transpose(down_weight)
    gain = norm_gain.reshape(1, model)
    dma = pltpu.SemaphoreType.DMA
    scratch = [
        pltpu.VMEM((nz, 3 * rows, 128), BF16),
        pltpu.VMEM((nz, 8, rows), F32),
        pltpu.VMEM((ny, 2 * rows, 128), BF16),
        pltpu.VMEM((nz, ny, 2 * wrows, ff), BF16),
        pltpu.VMEM((nz, ny, wrows, ff), BF16),
        pltpu.VMEM((256, model), BF16),
        pltpu.VMEM((share, model), BF16),
        pltpu.VMEM((1, model), F32),
        pltpu.VMEM((nz, 2, ny * rows, 128), F32),
        pltpu.VMEM((ny, ngroup, 8, ny * rows), F32),
        pltpu.VMEM((ny, rows, 256), BF16),
        pltpu.VMEM((ny, rows, 256), BF16),
        pltpu.VMEM((nt, share, model), BF16),
        pltpu.VMEM((nt, share, model), BF16),
        pltpu.VMEM((nt, share, model), BF16),
        pltpu.VMEM((share, model), F32),
        pltpu.VMEM((nt, share, model), BF16),
        pltpu.VMEM((nt, share, model), BF16),
        pltpu.VMEM((rows, ff), BF16),
        dma((9,)),
        dma((2, half + 1)), dma((2, half + 1)),
        dma((2, half + 1)), dma((2, half + 1)),
        dma((2, half + 1)), dma((2, half + 1)),
        dma((2, half + 1)), dma((2, half + 1)),
        dma((ny,)), dma((ny,)),
        dma((ny,)), dma((ny,)),
        dma((2, half + 1, 2)), dma((2, half + 1, 2)),
        dma((2, half + 1)), dma((2, half + 1)),
        dma((ngroup, ny)), dma((ngroup, ny)),
        dma((ny,)), dma((ny,)),
        dma((nt,)), dma((nt,)),
        dma((nt,)), dma((nt,)),
        dma((nt,)), dma((nt,)),
    ]
    return pl.pallas_call(
        functools.partial(layer_kernel, nz, ny, nt, rows, wrows, share),
        out_shape=jax.ShapeDtypeStruct((share, model), BF16),
        in_specs=[pl.BlockSpec(memory_space=pl.ANY)] * 9,
        out_specs=pl.BlockSpec(memory_space=pltpu.VMEM),
        scratch_shapes=scratch,
        compiler_params=pltpu.CompilerParams(
            collective_id=0, has_side_effects=True, vmem_limit_bytes=60 * 1024 * 1024
        ),
        name="layer",
    )(kv, off, q, gu, dt, stream, out_narrow, out_broad, gain)


def build(mesh, nz, ny, nt):
    torus = Mesh(mesh.devices.reshape(nz, ny, nt), SP_TP)
    in_specs = (
        P(SP, None),
        P(SP, "tp"),
        P(SP, "tp"),
        P(SP, "tp"),
        P(SP, "tp"),
        P(SP, "tp"),
        P(SP, "tp"),
        P(SP, "tp"),
        P("tp", None),
        P("tp", None),
        P(),
        P(SP, "tp"),
        P(SP, "tp"),
        P("tp", SP),
    )
    return jax.shard_map(
        functools.partial(local, nz, ny, nt),
        mesh=torus,
        in_specs=in_specs,
        out_specs=P(SP_TP, None),
        check_vma=False,
    )


def solution(mesh):
    sp = mesh.shape["sp"]
    ny = 4
    return build(mesh, sp // ny, ny, mesh.shape["tp"])
```

```python
import functools
import math

import jax
import jax.numpy as jnp
from jax import lax
from jax.experimental import pallas as pl
from jax.experimental.pallas import tpu as pltpu
from jax.sharding import Mesh
from jax.sharding import PartitionSpec as P

NARROW_SIZE = 64
BROAD_SIZE = 128
SP = ("sp_0", "sp_1")
SP_TP = ("sp_0", "sp_1", "tp")
MESH = pl.DeviceIdType.MESH
LOG2E = 1.4426950408889634
SCALE = (NARROW_SIZE**-0.5 * LOG2E, BROAD_SIZE**-0.5 * LOG2E)
norm_eps = 1e-06
F32 = jnp.float32
BF16 = jnp.bfloat16
NT = (((1,), (1,)), ((), ()))
NN = (((1,), (0,)), ((), ()))


def dot(a, b, dims=NN, precision=None):
    return lax.dot_general(a, b, dims, preferred_element_type=F32, precision=precision)


def wrap(value, size):
    return lax.rem(value + 2 * size, size)


def layer_kernel(
    nz, ny, nt, rows, wrows, share,
    stream_in, qn_in, qb_in, kn_in, kb_in, vn_in, vb_in, off_in, on_in, ob_in, gain_in,
    gate_in, up_in, down_in,
    out,
    kv, off, qs, w, on, ob, st, gain, obuf, tall, ar, ao, part, rs, nb, mid_s, part2, rs2,
    qn, tcol, trow,
    lsem, kvs, kvr, offs, offr, ws, wr, q_s, q_r, yas, yar, yrs, yrr,
    t_s, t_r, a_s, a_r, r1s, r1r, n_s, n_r, r2s, r2r,
):
    z = lax.axis_index("sp_0")
    y = lax.axis_index("sp_1")
    t = lax.axis_index("tp")
    up = (wrap(z + 1, nz), y, t)
    dn = (wrap(z - 1, nz), y, t)
    yp = (z, wrap(y + 1, ny), t)
    ym = (z, wrap(y - 1, ny), t)
    half = nz // 2
    narrow = qn.shape[1]

    def ypeer(j):
        return (z, wrap(y + j, ny), t)

    def toff(j):
        core = lax.rem(t, 2)
        return wrap(t - core + 2 * (j // 2), nt) + (core + j % 2 - 2 * core * (j % 2))

    def tpeer(j):
        return (z, y, toff(j))

    far = sorted(range(1, nt), key=lambda j: -min(j // 2, (nt - j) // 2 if j % 2 == 0 else (nt + 1 - j) // 2))

    def rc(src, dst, ssem, rsem, dev):
        return pltpu.make_async_remote_copy(
            src_ref=src, dst_ref=dst, send_sem=ssem, recv_sem=rsem,
            device_id=dev, device_id_type=MESH,
        )

    barrier = pltpu.get_barrier_semaphore()
    peers = [up, dn] + [ypeer(j) for j in range(1, ny)] + [tpeer(j) for j in range(1, nt)]
    for p in peers:
        pl.semaphore_signal(barrier, inc=1, device_id=p, device_id_type=MESH)

    pairs = [
        (kn_in, kv.at[z, 0, pl.ds(0, narrow), :]),
        (vn_in, kv.at[z, 0, pl.ds(narrow, narrow), :]),
        (kb_in, kv.at[z, 1]),
        (vb_in, kv.at[z, 2]),
        (off_in, off.at[z]),
        (qn_in, qs.at[y, pl.ds(0, narrow), :]),
        (qb_in, qs.at[y, pl.ds(narrow, rows), :]),
        (gate_in, w.at[z, y, pl.ds(0, wrows), :]),
        (up_in, w.at[z, y, pl.ds(wrows, wrows), :]),
        (down_in, w.at[z, y, pl.ds(2 * wrows, wrows), :]),
        (stream_in.at[pl.ds(t * share, share), :], st),
        (on_in, on),
        (ob_in, ob),
        (gain_in, gain),
    ]
    copies = [pltpu.make_async_copy(a, b, lsem.at[i]) for i, (a, b) in enumerate(pairs)]
    first, second = copies[:10], copies[10:]
    for c in copies:
        c.start()

    tcol[...] = jnp.zeros(tcol.shape, F32)

    def zero_body(i, carry):
        obuf[i] = jnp.zeros(obuf.shape[1:], F32)
        return carry

    lax.fori_loop(0, nz, zero_body, 0)
    for c in first:
        c.wait()
    pl.semaphore_wait(barrier, len(peers))

    def shard_z(d, k):
        return wrap(z - k, nz) if d == 0 else wrap(z + k, nz)

    def ring(ref, ssem, rsem, d):
        return rc(ref, ref, ssem, rsem, up if d == 0 else dn)

    def kv_ring(d, k, c):
        return ring(kv.at[shard_z(d, k - 1), c], kvs.at[d, k, c], kvr.at[d, k, c], d)

    def off_ring(d, k):
        return ring(off.at[shard_z(d, k - 1)], offs.at[d, k], offr.at[d, k], d)

    def w_ring(d, k):
        return ring(w.at[shard_z(d, k - 1), y], ws.at[d, k], wr.at[d, k], d)

    def w_y(d, k, e):
        ref = w.at[shard_z(d, k), y]
        return rc(ref, ref, yas.at[d, k, e], yar.at[d, k, e], yp if e == 0 else ym)

    def w_relay(d, k):
        src_y = wrap(y - 1, ny) if d == 0 else wrap(y + 1, ny)
        ref = w.at[shard_z(d, k), src_y]
        return rc(ref, ref, yrs.at[d, k], yrr.at[d, k], yp if d == 0 else ym)

    def q_send(j):
        return rc(qs.at[y], qs.at[y], q_s.at[j], q_r.at[j], ypeer(j))

    def t_send(g, j):
        ref = tall.at[y, g]
        return rc(ref, ref, t_s.at[g, j], t_r.at[g, j], ypeer(j))

    for j in range(1, ny):
        q_send(j).start()
    for d in range(2):
        off_ring(d, 1).start()
    for c in range(3):
        for d in range(2):
            kv_ring(d, 1, c).start()
    for d in range(2):
        w_ring(d, 1).start()
    for e in range(2):
        w_y(0, 0, e).start()

    nq = ny * rows
    key_row = lax.broadcasted_iota(jnp.int32, (2 * rows, 2 * rows), 0)
    key_col = lax.broadcasted_iota(jnp.int32, (2 * rows, 2 * rows), 1)
    same_block = lax.div(key_row, rows) == lax.div(key_col, rows)
    tri = jnp.where(jnp.logical_and(key_row > key_col, same_block), 1.0, 0.0).astype(BF16)
    pick_row = lax.broadcasted_iota(jnp.int32, (2 * rows, 128), 0)
    pick_col = lax.broadcasted_iota(jnp.int32, (2 * rows, 128), 1)

    def process(blocks, h, diag):
        nk = len(blocks) * rows
        if h == 0:
            keys = [kv[zz, 0, 0:narrow, :] for zz, _, _ in blocks]
            logits = dot(qn[...], jnp.concatenate(keys, axis=1))
        else:
            keys = [kv[zz, 1] for zz, _, _ in blocks]
            logits = dot(qs[:, narrow:, :].reshape(nq, 128), jnp.concatenate(keys, axis=0), NT)
        bias = [off[zz, h : h + 1, :] * LOG2E for zz, _, _ in blocks]
        if not diag:
            bias = [jnp.where(b[2], v, -1e30) for b, v in zip(blocks, bias)]
        logits = logits * SCALE[h] + jnp.concatenate(bias, axis=1)
        soft = jnp.maximum(jnp.log2(1.0 + jnp.exp2(jnp.minimum(logits, 126.0))), logits)
        if diag:
            q_pos = lax.broadcasted_iota(jnp.int32, (nq, rows), 0)
            k_pos = y * rows + lax.broadcasted_iota(jnp.int32, (nq, rows), 1)
            causal = k_pos < q_pos
            low = jnp.where(causal, soft, 0.0).astype(BF16)
        else:
            low = soft.astype(BF16)
        place = 2 * blocks[0][1] + h
        if len(blocks) > 1:
            place = jnp.where(pick_row < rows, place, 2 * blocks[1][1] + h)
        pick = jnp.where(pick_col == place, 1.0, 0.0).astype(BF16)
        tcol[...] += dot(low, pick[0:nk])
        weight = jnp.exp2(logits - soft - dot(low, tri[0:nk, 0:nk]))
        if diag:
            weight = jnp.where(causal, weight, 0.0)
        weight = weight.astype(BF16)
        base = h * narrow
        for i, (zz, s, _) in enumerate(blocks):
            vt = kv[zz, 0, narrow:, :] if h == 0 else jnp.transpose(kv[zz, 2])
            obuf[s, base : base + vt.shape[0], :] = dot(
                vt, weight[:, i * rows : (i + 1) * rows], NT
            )

    def pass_on(make, k):
        for d in range(2):
            def one(d=d):
                make(d, k).wait_recv()

                @pl.when(k < half - d)
                def _():
                    make(d, k + 1).start()

            if d == 0:
                one()
            else:
                pl.when(k < half)(one)

    def forward(k):
        pass_on(off_ring, k)
        for c in range(3):
            pass_on(lambda d, kk, c=c: kv_ring(d, kk, c), k)

    def forward_w(k):
        pass_on(w_ring, k)
        for e in range(2):
            w_y(0, k, e).start()

        @pl.when(k < half)
        def _():
            for e in range(2):
                w_y(1, k, e).start()

    def forward_body(k, carry):
        forward(k)
        return carry

    lax.fori_loop(1, 3, forward_body, 0)
    forward_w(jnp.int32(1))
    for j in range(1, ny):
        q_send(j).wait_recv()
    for i in range(ny):
        head = jnp.transpose(qs[i, 0:narrow, :].astype(F32))
        qn[i * rows : (i + 1) * rows, :] = head.astype(BF16)
    for h in range(2):
        process([(z, jnp.int32(0), None)], h, True)

    def kv_step(k, carry):
        pl.when(k >= 3)(functools.partial(forward, k))
        blocks = [
            (wrap(z - k, nz), 2 * k - 1, k <= z),
            (wrap(z + k, nz), 2 * k, jnp.logical_and(k < half, z + k >= nz)),
        ]
        pl.when(k <= z)(functools.partial(process, blocks, 0, False))
        pl.when(k >= 3)(functools.partial(forward_w, k - 1))
        pl.when(k <= z)(functools.partial(process, blocks, 1, False))

        @pl.when(lax.rem(k, 2) == 0)
        def _():
            g = lax.div(k, 2) - 1
            trow[...] = jnp.transpose(tcol[...])
            tall[y, g] = trow[pl.ds(pl.multiple_of(8 * g, 8), 8), :]
            for j in range(1, ny):
                t_send(g, j).start()

        return carry

    lax.fori_loop(1, half + 1, kv_step, 0)

    ngroup = nz // 4
    for g in range(ngroup):
        for j in range(1, ny):
            t_send(g, j).wait_recv()

    trows = ny * ngroup * 8
    nrow = 2 * nz
    flat = tall[...].reshape(trows, nq)
    fr = lax.broadcasted_iota(jnp.int32, (nrow, trows), 0)
    fc = lax.broadcasted_iota(jnp.int32, (nrow, trows), 1)

    def slot_z(slot):
        k = lax.shift_right_logical(slot + 1, 1)
        signed = jnp.where(lax.bitwise_and(slot, 1) == 1, -k, k)
        return lax.bitwise_and(z + signed + nz, nz - 1)

    per_y = ngroup * 8
    c_y = lax.div(fc, per_y)
    c_in = lax.rem(fc, per_y)
    r_order = slot_z(lax.shift_right_logical(fr, 1)) * ny + y
    c_order = slot_z(lax.shift_right_logical(c_in, 1)) * ny + c_y
    same = lax.bitwise_and(fr, 1) == lax.bitwise_and(c_in, 1)
    sel = jnp.where(jnp.logical_and(same, c_order > r_order), 1.0, 0.0).astype(F32)
    later = dot(sel, flat, NN, lax.Precision.HIGHEST)
    factor = jnp.exp2(-later)
    for rb in range(ny):
        cols = slice(rb * rows, (rb + 1) * rows)
        for lo, hi, h in ((0, narrow, 0), (narrow, narrow + 128, 1)):
            acc = jnp.zeros((hi - lo, rows), F32)
            for s in range(nz):
                row = factor[2 * s + h : 2 * s + h + 1, cols]
                acc = acc + row * obuf[s, lo:hi, cols]
            ao[rb, lo:hi, :] = acc.astype(BF16)

    def a_send(j):
        peer = wrap(y + j, ny)
        return rc(ao.at[peer], ar.at[j], a_s.at[j], a_r.at[j], ypeer(j))

    for j in range(1, ny):
        a_send(j).start()
    forward_w(jnp.int32(half))
    for k in range(half):
        w_y(0, k, 0).wait_recv()
        w_relay(0, k).start()
        if k >= 1:
            w_y(1, k, 1).wait_recv()
            w_relay(1, k).start()
    for c in second:
        c.wait()
    attended = ao[y].astype(F32)
    for j in range(1, ny):
        a_send(j).wait_recv()
        attended = attended + ar[j].astype(F32)
    att_n = jnp.transpose(attended[0:narrow, :]).astype(BF16)
    att_b = jnp.transpose(attended[narrow : narrow + 128, :]).astype(BF16)
    model = out.shape[1]
    for c in range(model // 512):
        cols = slice(c * 512, (c + 1) * 512)
        block = (dot(att_n, on[:, cols]) + dot(att_b, ob[:, cols])).astype(BF16)
        part[:, :, cols] = block.reshape(nt, share, 512)

    def r1_send(j):
        return rc(part.at[toff(j)], rs.at[j], r1s.at[j], r1r.at[j], tpeer(j))

    for j in far:
        r1_send(j).start()
    w_y(0, half, 0).wait_recv()
    w_relay(0, half).start()
    total = st[...].astype(F32) + part[t].astype(F32)
    for j in range(1, nt):
        r1_send(j).wait_recv()
        total = total + rs[j].astype(F32)
    mid = total.astype(BF16).astype(F32)
    mid_s[...] = mid
    normed = mid * lax.rsqrt(jnp.mean(mid * mid, axis=1, keepdims=True) + norm_eps) * gain[...]
    nb[t] = normed.astype(BF16)

    def n_send(j):
        return rc(nb.at[t], nb.at[t], n_s.at[j], n_r.at[j], tpeer(j))

    for j in far:
        n_send(j).start()

    def w_wait(k, d):
        if d == 0:
            w_y(0, k, 1).wait_recv()
            w_relay(0, k).wait_recv()
        else:
            w_y(1, k, 0).wait_recv()
            w_relay(1, k).wait_recv()

    def w_wait_body(k, carry):
        w_wait(k, 0)

        @pl.when(jnp.logical_and(k >= 1, k < half))
        def _():
            w_wait(k, 1)

        return carry

    lax.fori_loop(0, half + 1, w_wait_body, 0)
    for j in range(1, nt):
        n_send(j).wait_recv()
    gate = jnp.zeros((rows, w.shape[3]), F32)
    upv = jnp.zeros((rows, w.shape[3]), F32)
    span = ny * wrows
    for zz in range(nz):
        lhs = nb[:, :, zz * span : (zz + 1) * span].reshape(rows, span)
        gate = gate + dot(lhs, w[zz, :, 0:wrows, :].reshape(span, w.shape[3]))
        upv = upv + dot(lhs, w[zz, :, wrows : 2 * wrows, :].reshape(span, w.shape[3]))
    hidden = (gate / (1.0 + jnp.exp(-gate)) * upv).astype(BF16)
    for zz in range(nz):
        rhs = w[zz, :, 2 * wrows :, :].reshape(span, w.shape[3])
        block = dot(hidden, rhs, NT).astype(BF16)
        part2[:, :, zz * span : (zz + 1) * span] = block.reshape(nt, share, span)

    def r2_send(j):
        return rc(part2.at[toff(j)], rs2.at[j], r2s.at[j], r2r.at[j], tpeer(j))

    for j in far:
        r2_send(j).start()

    def drain(k, carry):
        for d in range(2):
            @pl.when(k <= half - d)
            def _():
                for c in range(3):
                    kv_ring(d, k, c).wait_send()
                off_ring(d, k).wait_send()
                w_ring(d, k).wait_send()
                for e in range(2):
                    w_y(d, k, e).wait_send()
                w_relay(d, k).wait_send()
        return carry

    lax.fori_loop(1, half + 1, drain, 0)
    for e in range(2):
        w_y(0, 0, e).wait_send()
    w_relay(0, 0).wait_send()
    for j in range(1, ny):
        q_send(j).wait_send()
        a_send(j).wait_send()
        for g in range(ngroup):
            t_send(g, j).wait_send()
    for j in range(1, nt):
        r1_send(j).wait_send()
        n_send(j).wait_send()
    total = mid_s[...] + part2[t].astype(F32)
    for j in range(1, nt):
        r2_send(j).wait_recv()
        total = total + rs2[j].astype(F32)
    out[...] = total.astype(BF16)
    for j in range(1, nt):
        r2_send(j).wait_send()


def local(
    nz, ny, nt,
    stream, query_narrow, query_broad, key_narrow, key_broad, value_narrow, value_broad,
    key_offsets, out_narrow, out_broad, norm_gain, gate_weight, up_weight, down_weight,
):
    rows, model = stream.shape
    wrows, ff = gate_weight.shape
    share = rows // nt
    half = nz // 2
    ngroup = nz // 4
    gain = norm_gain.reshape(1, model)
    dma = pltpu.SemaphoreType.DMA
    scratch = [
        pltpu.VMEM((nz, 3, rows, 128), BF16),
        pltpu.VMEM((nz, 2, rows), F32),
        pltpu.VMEM((ny, 192, 128), BF16),
        pltpu.VMEM((nz, ny, 3 * wrows, ff), BF16),
        pltpu.VMEM((64, model), BF16),
        pltpu.VMEM((128, model), BF16),
        pltpu.VMEM((share, model), BF16),
        pltpu.VMEM((1, model), F32),
        pltpu.VMEM((nz + 1, 192, ny * rows), F32),
        pltpu.VMEM((ny, ngroup, 8, ny * rows), F32),
        pltpu.VMEM((ny, 192, rows), BF16),
        pltpu.VMEM((ny, 192, rows), BF16),
        pltpu.VMEM((nt, share, model), BF16),
        pltpu.VMEM((nt, share, model), BF16),
        pltpu.VMEM((nt, share, model), BF16),
        pltpu.VMEM((share, model), F32),
        pltpu.VMEM((nt, share, model), BF16),
        pltpu.VMEM((nt, share, model), BF16),
        pltpu.VMEM((ny * rows, 64), BF16),
        pltpu.VMEM((ny * rows, 128), F32),
        pltpu.VMEM((128, ny * rows), F32),
        dma((14,)),
        dma((2, half + 1, 3)), dma((2, half + 1, 3)),
        dma((2, half + 1)), dma((2, half + 1)),
        dma((2, half + 1)), dma((2, half + 1)),
        dma((ny,)), dma((ny,)),
        dma((2, half + 1, 2)), dma((2, half + 1, 2)),
        dma((2, half + 1)), dma((2, half + 1)),
        dma((ngroup, ny)), dma((ngroup, ny)),
        dma((ny,)), dma((ny,)),
        dma((nt,)), dma((nt,)),
        dma((nt,)), dma((nt,)),
        dma((nt,)), dma((nt,)),
    ]
    return pl.pallas_call(
        functools.partial(layer_kernel, nz, ny, nt, rows, wrows, share),
        out_shape=jax.ShapeDtypeStruct((share, model), BF16),
        in_specs=[pl.BlockSpec(memory_space=pl.ANY)] * 14,
        out_specs=pl.BlockSpec(memory_space=pltpu.VMEM),
        scratch_shapes=scratch,
        compiler_params=pltpu.CompilerParams(
            collective_id=0, has_side_effects=True, vmem_limit_bytes=60 * 1024 * 1024
        ),
        name="layer",
    )(
        stream, query_narrow.T, query_broad, key_narrow.T, key_broad, value_narrow.T, value_broad,
        key_offsets.T, out_narrow, out_broad, gain, gate_weight, up_weight, down_weight.T,
    )


def build(mesh, nz, ny, nt):
    torus = Mesh(mesh.devices.reshape(nz, ny, nt), SP_TP)
    in_specs = (
        P(SP, None),
        P(SP, "tp"),
        P(SP, "tp"),
        P(SP, "tp"),
        P(SP, "tp"),
        P(SP, "tp"),
        P(SP, "tp"),
        P(SP, "tp"),
        P("tp", None),
        P("tp", None),
        P(),
        P(SP, "tp"),
        P(SP, "tp"),
        P("tp", SP),
    )
    return jax.shard_map(
        functools.partial(local, nz, ny, nt),
        mesh=torus,
        in_specs=in_specs,
        out_specs=P(SP_TP, None),
        check_vma=False,
    )


def solution(mesh):
    sp = mesh.shape["sp"]
    ny = 4
    return build(mesh, sp // ny, ny, mesh.shape["tp"])
```

```python
import functools
import math

import jax
import jax.numpy as jnp
from jax import lax
from jax.experimental import pallas as pl
from jax.experimental.pallas import tpu as pltpu
from jax.sharding import Mesh
from jax.sharding import PartitionSpec as P

NARROW_SIZE = 64
BROAD_SIZE = 128
SP = ("sp_0", "sp_1")
SP_TP = ("sp_0", "sp_1", "tp")
MESH = pl.DeviceIdType.MESH
LOG2E = 1.4426950408889634
SCALE = (NARROW_SIZE**-0.5 * LOG2E, BROAD_SIZE**-0.5 * LOG2E)
norm_eps = 1e-06
F32 = jnp.float32
BF16 = jnp.bfloat16
NT = (((1,), (1,)), ((), ()))
NN = (((1,), (0,)), ((), ()))


def dot(a, b, dims=NN, precision=None):
    return lax.dot_general(a, b, dims, preferred_element_type=F32, precision=precision)


def wrap(value, size):
    return lax.rem(value + 2 * size, size)


def layer_kernel(
    nz, ny, nt, rows, wrows, share,
    stream_in, qn_in, qb_in, kn_in, kb_in, vn_in, vb_in, off_in, on_in, ob_in, gain_in,
    gate_in, up_in, down_in,
    out,
    kv, off, qs, w, ow, st, gain, obuf, tall, ar, ao, att, nb, part2, rs2,
    qn, tcol, trow, fac,
    lsem, kvs, kvr, offs, offr, ws, wr, q_s, q_r, yas, yar, yrs, yrr,
    t_s, t_r, a_s, a_r, ows, owr, n_s, n_r, r2s, r2r,
):
    z = lax.axis_index("sp_0")
    y = lax.axis_index("sp_1")
    t = lax.axis_index("tp")
    up = (wrap(z + 1, nz), y, t)
    dn = (wrap(z - 1, nz), y, t)
    yp = (z, wrap(y + 1, ny), t)
    ym = (z, wrap(y - 1, ny), t)
    half = nz // 2
    narrow = qn.shape[1]

    def ypeer(j):
        return (z, wrap(y + j, ny), t)

    def toff(j):
        core = lax.rem(t, 2)
        return wrap(t - core + 2 * (j // 2), nt) + (core + j % 2 - 2 * core * (j % 2))

    def tpeer(j):
        return (z, y, toff(j))

    far = sorted(range(1, nt), key=lambda j: -min(j // 2, (nt - j) // 2 if j % 2 == 0 else (nt + 1 - j) // 2))

    def rc(src, dst, ssem, rsem, dev):
        return pltpu.make_async_remote_copy(
            src_ref=src, dst_ref=dst, send_sem=ssem, recv_sem=rsem,
            device_id=dev, device_id_type=MESH,
        )

    barrier = pltpu.get_barrier_semaphore()
    peers = [up, dn] + [ypeer(j) for j in range(1, ny)] + [tpeer(j) for j in range(1, nt)]
    for p in peers:
        pl.semaphore_signal(barrier, inc=1, device_id=p, device_id_type=MESH)

    pairs = [
        (kn_in, kv.at[z, 0, pl.ds(0, narrow), :]),
        (vn_in, kv.at[z, 0, pl.ds(narrow, narrow), :]),
        (kb_in, kv.at[z, 1]),
        (vb_in, kv.at[z, 2]),
        (off_in, off.at[z]),
        (qn_in, qs.at[y, pl.ds(0, narrow), :]),
        (qb_in, qs.at[y, pl.ds(narrow, rows), :]),
        (gate_in, w.at[z, y, pl.ds(0, wrows), :]),
        (up_in, w.at[z, y, pl.ds(wrows, wrows), :]),
        (down_in, w.at[z, y, pl.ds(2 * wrows, wrows), :]),
        (on_in, ow.at[t, pl.ds(0, narrow), :]),
        (ob_in, ow.at[t, pl.ds(narrow, rows), :]),
        (stream_in, st),
        (gain_in, gain),
    ]
    copies = [pltpu.make_async_copy(a, b, lsem.at[i]) for i, (a, b) in enumerate(pairs)]
    first, second, third = copies[:10], copies[10:12], copies[12:]
    for c in copies:
        c.start()

    for c in first:
        c.wait()
    pl.semaphore_wait(barrier, len(peers))

    def shard_z(d, k):
        return wrap(z - k, nz) if d == 0 else wrap(z + k, nz)

    def ring(ref, ssem, rsem, d):
        return rc(ref, ref, ssem, rsem, up if d == 0 else dn)

    def kv_ring(d, k, c):
        return ring(kv.at[shard_z(d, k - 1), c], kvs.at[d, k, c], kvr.at[d, k, c], d)

    def off_ring(d, k):
        return ring(off.at[shard_z(d, k - 1)], offs.at[d, k], offr.at[d, k], d)

    def w_ring(d, k):
        return ring(w.at[shard_z(d, k - 1), y], ws.at[d, k], wr.at[d, k], d)

    def w_y(d, k, e):
        ref = w.at[shard_z(d, k), y]
        return rc(ref, ref, yas.at[d, k, e], yar.at[d, k, e], yp if e == 0 else ym)

    def w_relay(d, k):
        src_y = wrap(y - 1, ny) if d == 0 else wrap(y + 1, ny)
        ref = w.at[shard_z(d, k), src_y]
        return rc(ref, ref, yrs.at[d, k], yrr.at[d, k], yp if d == 0 else ym)

    def q_send(j):
        return rc(qs.at[y], qs.at[y], q_s.at[j], q_r.at[j], ypeer(j))

    partner = toff(1)
    xp, xm, xo = toff(2), toff(nt - 2), toff(nt // 2)
    core = lax.rem(t, 2)
    nx = nt // 2

    def ow_send(i):
        src, dst = (
            (t, partner), (t, xp), (t, xm),
            (xm, partner), (xp, partner),
            (jnp.where(core == 0, xm, xp), jnp.where(core == 0, xp, xm)),
            (xo, partner),
        )[i]
        return rc(ow.at[src], ow.at[src], ows.at[i], owr.at[i], (z, y, dst))

    def t_send(g, j):
        ref = tall.at[y, g]
        return rc(ref, ref, t_s.at[g, j], t_r.at[g, j], ypeer(j))

    for j in range(1, ny):
        q_send(j).start()
    for d in range(2):
        off_ring(d, 1).start()
    for c in range(3):
        for d in range(2):
            kv_ring(d, 1, c).start()
    for d in range(2):
        w_ring(d, 1).start()
    for e in range(2):
        w_y(0, 0, e).start()
    for c in second:
        c.wait()
    if nx > 2:
        ow_send(1).start()
        ow_send(2).start()
    ow_send(0).start()

    tcol[...] = jnp.zeros(tcol.shape, F32)

    def zero_body(i, carry):
        obuf[i] = jnp.zeros(obuf.shape[1:], F32)
        return carry

    lax.fori_loop(0, nz + 1, zero_body, 0)
    nq = ny * rows
    key_row = lax.broadcasted_iota(jnp.int32, (2 * rows, 2 * rows), 0)
    key_col = lax.broadcasted_iota(jnp.int32, (2 * rows, 2 * rows), 1)
    same_block = lax.div(key_row, rows) == lax.div(key_col, rows)
    tri = jnp.where(jnp.logical_and(key_row > key_col, same_block), 1.0, 0.0).astype(BF16)
    pick_row = lax.broadcasted_iota(jnp.int32, (2 * rows, 128), 0)
    pick_col = lax.broadcasted_iota(jnp.int32, (2 * rows, 128), 1)

    def process(blocks, h, diag):
        nk = len(blocks) * rows
        if h == 0:
            keys = [kv[zz, 0, 0:narrow, :] for zz, _, _ in blocks]
            logits = dot(qn[...], jnp.concatenate(keys, axis=1))
        else:
            keys = [kv[zz, 1] for zz, _, _ in blocks]
            logits = dot(qs[:, narrow:, :].reshape(nq, 128), jnp.concatenate(keys, axis=0), NT)
        bias = [off[zz, h : h + 1, :] * LOG2E for zz, _, _ in blocks]
        if not diag:
            bias = [jnp.where(b[2], v, -1e30) for b, v in zip(blocks, bias)]
        logits = logits * SCALE[h] + jnp.concatenate(bias, axis=1)
        soft = jnp.maximum(jnp.log2(1.0 + jnp.exp2(jnp.minimum(logits, 126.0))), logits)
        if diag:
            q_pos = lax.broadcasted_iota(jnp.int32, (nq, rows), 0)
            k_pos = y * rows + lax.broadcasted_iota(jnp.int32, (nq, rows), 1)
            causal = k_pos < q_pos
            low = jnp.where(causal, soft, 0.0).astype(BF16)
        else:
            low = soft.astype(BF16)
        place = 2 * blocks[0][1] + h
        if len(blocks) > 1:
            place = jnp.where(pick_row < rows, place, 2 * blocks[1][1] + h)
        pick = jnp.where(pick_col == place, 1.0, 0.0).astype(BF16)
        tcol[...] += dot(low, pick[0:nk])
        weight = jnp.exp2(logits - soft - dot(low, tri[0:nk, 0:nk]))
        if diag:
            weight = jnp.where(causal, weight, 0.0)
        weight = weight.astype(BF16)
        base = h * narrow
        for i, (zz, s, _) in enumerate(blocks):
            vt = kv[zz, 0, narrow:, :] if h == 0 else jnp.transpose(kv[zz, 2])
            obuf[s, base : base + vt.shape[0], :] = dot(
                vt, weight[:, i * rows : (i + 1) * rows], NT
            )

    def pass_on(make, k):
        for d in range(2):
            def one(d=d):
                make(d, k).wait_recv()

                @pl.when(k < half - d)
                def _():
                    make(d, k + 1).start()

            if d == 0:
                one()
            else:
                pl.when(k < half)(one)

    def forward(k):
        pass_on(off_ring, k)
        for c in range(3):
            pass_on(lambda d, kk, c=c: kv_ring(d, kk, c), k)

    def w_sides(k):
        for e in range(2):
            w_y(0, k, e).start()

        @pl.when(k < half)
        def _():
            for e in range(2):
                w_y(1, k, e).start()

    def relay(d, k):
        w_y(d, k, d).wait_recv()
        w_relay(d, k).start()

    def forward_body(k, carry):
        forward(k)
        return carry

    lax.fori_loop(1, 3, forward_body, 0)
    pass_on(w_ring, jnp.int32(1))
    w_sides(jnp.int32(1))
    relay(0, 0)
    for j in range(1, ny):
        q_send(j).wait_recv()
    for i in range(ny):
        head = jnp.transpose(qs[i, 0:narrow, :].astype(F32))
        qn[i * rows : (i + 1) * rows, :] = head.astype(BF16)
    for h in range(2):
        process([(z, jnp.int32(0), None)], h, True)

    def kv_step(k, carry):
        pl.when(k >= 3)(functools.partial(forward, k))
        blocks = [
            (wrap(z - k, nz), 2 * k - 1, k <= z),
            (wrap(z + k, nz), 2 * k, jnp.logical_and(k < half, z + k >= nz)),
        ]
        pl.when(k <= z)(functools.partial(process, blocks, 0, False))

        @pl.when(k >= 3)
        def _():
            pass_on(w_ring, k - 1)
            pl.when(k < half)(functools.partial(w_sides, k - 1))

        @pl.when(jnp.logical_and(k > 3, k < half))
        def _():
            relay(0, k - 3)
            relay(1, k - 3)

        if nx > 2:
            @pl.when(k == half - 2)
            def _():
                ow_send(1).wait_recv()
                ow_send(2).wait_recv()
                ow_send(5).start()
                ow_send(3).start()
                ow_send(4).start()

        pl.when(k <= z)(functools.partial(process, blocks, 1, False))

        @pl.when(lax.rem(k, 2) == 0)
        def _():
            g = lax.div(k, 2) - 1
            trow[...] = jnp.transpose(tcol[...])
            tall[y, g] = trow[pl.ds(pl.multiple_of(8 * g, 8), 8), :]
            for j in range(1, ny):
                t_send(g, j).start()

        return carry

    lax.fori_loop(1, half + 1, kv_step, 0)

    ngroup = nz // 4
    for g in range(ngroup):
        for j in range(1, ny):
            t_send(g, j).wait_recv()

    trows = ny * ngroup * 8
    nrow = 2 * nz
    flat = tall[...].reshape(trows, nq)
    fr = lax.broadcasted_iota(jnp.int32, (nrow, trows), 0)
    fc = lax.broadcasted_iota(jnp.int32, (nrow, trows), 1)

    def slot_z(slot):
        k = lax.shift_right_logical(slot + 1, 1)
        signed = jnp.where(lax.bitwise_and(slot, 1) == 1, -k, k)
        return lax.bitwise_and(z + signed + nz, nz - 1)

    per_y = ngroup * 8
    c_y = lax.div(fc, per_y)
    c_in = lax.rem(fc, per_y)
    r_order = slot_z(lax.shift_right_logical(fr, 1)) * ny + y
    c_order = slot_z(lax.shift_right_logical(c_in, 1)) * ny + c_y
    same = lax.bitwise_and(fr, 1) == lax.bitwise_and(c_in, 1)
    sel = jnp.where(jnp.logical_and(same, c_order > r_order), 1.0, 0.0).astype(F32)
    later = dot(sel, flat, NN, lax.Precision.HIGHEST)
    fac[...] = jnp.exp2(-later)

    def a_send(j):
        peer = wrap(y + j, ny)
        return rc(ao.at[peer], ar.at[j], a_s.at[j], a_r.at[j], ypeer(j))

    for j in (2, 1, 3, 0) if ny > 2 else range(ny - 1, -1, -1):
        rb = wrap(y + j, ny)
        cols = pl.ds(pl.multiple_of(rb * rows, rows), rows)
        for lo, hi, h in ((0, narrow, 0), (narrow, narrow + 128, 1)):
            acc = jnp.zeros((hi - lo, rows), F32)
            for s in range(nz):
                acc = acc + fac[2 * s + h : 2 * s + h + 1, cols] * obuf[s, lo:hi, cols]
            ao[rb, lo:hi, :] = acc.astype(BF16)
        if j > 0:
            a_send(j).start()
    pass_on(w_ring, jnp.int32(half))
    w_sides(jnp.int32(half - 1))
    w_sides(jnp.int32(half))
    early = max(half - 3, 1)
    for k in range(early, half - 1):
        relay(0, k)
        if k >= 1:
            relay(1, k)
    if nx > 2:
        ow_send(5).wait_recv()
        ow_send(6).start()
    attended = ao[y].astype(F32)
    for j in range(1, ny):
        a_send(j).wait_recv()
        attended = attended + ar[j].astype(F32)
    att[t] = attended.astype(BF16)

    def n_send(j):
        return rc(att.at[t], att.at[t], n_s.at[j], n_r.at[j], tpeer(j))

    for j in far:
        n_send(j).start()
    relay(0, half - 1)
    relay(1, half - 1)
    relay(0, half)
    for c in third:
        c.wait()
    ow_send(0).wait_recv()
    if nx > 2:
        for i in (3, 4, 6):
            ow_send(i).wait_recv()
    for j in range(1, nt):
        n_send(j).wait_recv()
    model = out.shape[1]
    square = jnp.zeros((rows, 1), F32)
    heads = [jnp.transpose(att[i]) for i in range(nt)]
    for c in range(model // 512):
        cols = slice(c * 512, (c + 1) * 512)
        block = st[:, cols].astype(F32)
        for i in range(nt):
            block = block + dot(heads[i], ow[i, :, cols])
        block = block.astype(BF16)
        st[:, cols] = block
        wide = block.astype(F32)
        square = square + jnp.sum(wide * wide, axis=1, keepdims=True)
    inverse = lax.rsqrt(square * (1.0 / model) + norm_eps)
    for c in range(model // 512):
        cols = slice(c * 512, (c + 1) * 512)
        nb[:, cols] = (st[:, cols].astype(F32) * inverse * gain[:, cols]).astype(BF16)

    def w_wait(k, d):
        if d == 0:
            w_y(0, k, 1).wait_recv()
            w_relay(0, k).wait_recv()
        else:
            w_y(1, k, 0).wait_recv()
            w_relay(1, k).wait_recv()

    def w_wait_body(k, carry):
        w_wait(k, 0)

        @pl.when(jnp.logical_and(k >= 1, k < half))
        def _():
            w_wait(k, 1)

        return carry

    lax.fori_loop(0, half + 1, w_wait_body, 0)
    gate = jnp.zeros((rows, w.shape[3]), F32)
    upv = jnp.zeros((rows, w.shape[3]), F32)
    span = ny * wrows
    for zz in range(nz):
        lhs = nb[:, zz * span : (zz + 1) * span]
        gate = gate + dot(lhs, w[zz, :, 0:wrows, :].reshape(span, w.shape[3]))
        upv = upv + dot(lhs, w[zz, :, wrows : 2 * wrows, :].reshape(span, w.shape[3]))
    hidden = (gate / (1.0 + jnp.exp(-gate)) * upv).astype(BF16)
    def r2_send(hf, j):
        return rc(
            part2.at[hf, toff(j)], rs2.at[hf, j], r2s.at[hf, j], r2r.at[hf, j], tpeer(j)
        )

    for hf in range(2):
        for i in range(nz // 2):
            zz = hf * (nz // 2) + i
            rhs = w[zz, :, 2 * wrows :, :].reshape(span, w.shape[3])
            block = dot(hidden, rhs, NT).astype(BF16)
            part2[hf, :, :, i * span : (i + 1) * span] = block.reshape(nt, share, span)
        for j in far:
            r2_send(hf, j).start()

    def drain(k, carry):
        for d in range(2):
            @pl.when(k <= half - d)
            def _():
                for c in range(3):
                    kv_ring(d, k, c).wait_send()
                off_ring(d, k).wait_send()
                w_ring(d, k).wait_send()
                for e in range(2):
                    w_y(d, k, e).wait_send()
                w_relay(d, k).wait_send()
        return carry

    lax.fori_loop(1, half + 1, drain, 0)
    for e in range(2):
        w_y(0, 0, e).wait_send()
    w_relay(0, 0).wait_send()
    for j in range(1, ny):
        q_send(j).wait_send()
        a_send(j).wait_send()
        for g in range(ngroup):
            t_send(g, j).wait_send()
    for j in range(1, nt):
        n_send(j).wait_send()
    ow_send(0).wait_send()
    if nx > 2:
        for i in range(1, 7):
            ow_send(i).wait_send()
    mine = pl.ds(pl.multiple_of(t * share, share), share)
    for hf in range(2):
        cols = slice(hf * model // 2, (hf + 1) * model // 2)
        total = st[mine, cols].astype(F32) + part2[hf, t].astype(F32)
        for j in range(1, nt):
            r2_send(hf, j).wait_recv()
            total = total + rs2[hf, j].astype(F32)
        out[:, cols] = total.astype(BF16)
    for hf in range(2):
        for j in range(1, nt):
            r2_send(hf, j).wait_send()


def local(
    nz, ny, nt,
    stream, query_narrow, query_broad, key_narrow, key_broad, value_narrow, value_broad,
    key_offsets, out_narrow, out_broad, norm_gain, gate_weight, up_weight, down_weight,
):
    rows, model = stream.shape
    wrows, ff = gate_weight.shape
    share = rows // nt
    half = nz // 2
    ngroup = nz // 4
    gain = norm_gain.reshape(1, model)
    dma = pltpu.SemaphoreType.DMA
    scratch = [
        pltpu.VMEM((nz, 3, rows, 128), BF16),
        pltpu.VMEM((nz, 2, rows), F32),
        pltpu.VMEM((ny, 192, 128), BF16),
        pltpu.VMEM((nz, ny, 3 * wrows, ff), BF16),
        pltpu.VMEM((nt, 192, model), BF16),
        pltpu.VMEM((rows, model), BF16),
        pltpu.VMEM((1, model), F32),
        pltpu.VMEM((nz + 1, 192, ny * rows), F32),
        pltpu.VMEM((ny, ngroup, 8, ny * rows), F32),
        pltpu.VMEM((ny, 192, rows), BF16),
        pltpu.VMEM((ny, 192, rows), BF16),
        pltpu.VMEM((nt, 192, rows), BF16),
        pltpu.VMEM((rows, model), BF16),
        pltpu.VMEM((2, nt, share, model // 2), BF16),
        pltpu.VMEM((2, nt, share, model // 2), BF16),
        pltpu.VMEM((ny * rows, 64), BF16),
        pltpu.VMEM((ny * rows, 128), F32),
        pltpu.VMEM((128, ny * rows), F32),
        pltpu.VMEM((2 * nz, ny * rows), F32),
        dma((14,)),
        dma((2, half + 1, 3)), dma((2, half + 1, 3)),
        dma((2, half + 1)), dma((2, half + 1)),
        dma((2, half + 1)), dma((2, half + 1)),
        dma((ny,)), dma((ny,)),
        dma((2, half + 1, 2)), dma((2, half + 1, 2)),
        dma((2, half + 1)), dma((2, half + 1)),
        dma((ngroup, ny)), dma((ngroup, ny)),
        dma((ny,)), dma((ny,)),
        dma((7,)), dma((7,)),
        dma((nt,)), dma((nt,)),
        dma((2, nt)), dma((2, nt)),
    ]
    return pl.pallas_call(
        functools.partial(layer_kernel, nz, ny, nt, rows, wrows, share),
        out_shape=jax.ShapeDtypeStruct((share, model), BF16),
        in_specs=[pl.BlockSpec(memory_space=pl.ANY)] * 14,
        out_specs=pl.BlockSpec(memory_space=pltpu.VMEM),
        scratch_shapes=scratch,
        compiler_params=pltpu.CompilerParams(
            collective_id=0, has_side_effects=True, vmem_limit_bytes=60 * 1024 * 1024
        ),
        name="layer",
    )(
        stream, query_narrow.T, query_broad, key_narrow.T, key_broad, value_narrow.T, value_broad,
        key_offsets.T, out_narrow, out_broad, gain, gate_weight, up_weight, down_weight.T,
    )


def build(mesh, nz, ny, nt):
    torus = Mesh(mesh.devices.reshape(nz, ny, nt), SP_TP)
    in_specs = (
        P(SP, None),
        P(SP, "tp"),
        P(SP, "tp"),
        P(SP, "tp"),
        P(SP, "tp"),
        P(SP, "tp"),
        P(SP, "tp"),
        P(SP, "tp"),
        P("tp", None),
        P("tp", None),
        P(),
        P(SP, "tp"),
        P(SP, "tp"),
        P("tp", SP),
    )
    return jax.shard_map(
        functools.partial(local, nz, ny, nt),
        mesh=torus,
        in_specs=in_specs,
        out_specs=P(SP_TP, None),
        check_vma=False,
    )


def solution(mesh):
    sp = mesh.shape["sp"]
    ny = 4
    return build(mesh, sp // ny, ny, mesh.shape["tp"])
```

```python
import functools
import math

import jax
import jax.numpy as jnp
from jax import lax
from jax.experimental import pallas as pl
from jax.experimental.pallas import tpu as pltpu
from jax.sharding import Mesh
from jax.sharding import PartitionSpec as P

NARROW_SIZE = 64
BROAD_SIZE = 128
SP = ("sp_0", "sp_1")
SP_TP = ("sp_0", "sp_1", "tp")
MESH = pl.DeviceIdType.MESH
LOG2E = 1.4426950408889634
SCALE = (NARROW_SIZE**-0.5 * LOG2E, BROAD_SIZE**-0.5 * LOG2E)
norm_eps = 1e-06
F32 = jnp.float32
BF16 = jnp.bfloat16
NT = (((1,), (1,)), ((), ()))
NN = (((1,), (0,)), ((), ()))


def dot(a, b, dims=NN, precision=None):
    return lax.dot_general(a, b, dims, preferred_element_type=F32, precision=precision)


def wrap(value, size):
    return lax.rem(value + 2 * size, size)


def layer_kernel(
    nz, ny, nt, rows, wrows, share,
    stream_in, qn_in, qb_in, kn_in, kb_in, vn_in, vb_in, off_in, on_in, ob_in, gain_in,
    gate_in, up_in, down_in,
    out,
    kv, off, qs, w, ow, st, gain, obuf, tall, ar, ao, att, nb, part2, rs2,
    qn, tcol, trow, fac, acc, lowb, gap,
    lsem, kvs, kvr, offs, offr, ws, wr, q_s, q_r, yas, yar, yrs, yrr,
    t_s, t_r, a_s, a_r, ows, owr, n_s, n_r, r2s, r2r,
):
    z = lax.axis_index("sp_0")
    y = lax.axis_index("sp_1")
    t = lax.axis_index("tp")
    up = (wrap(z + 1, nz), y, t)
    dn = (wrap(z - 1, nz), y, t)
    yp = (z, wrap(y + 1, ny), t)
    ym = (z, wrap(y - 1, ny), t)
    half = nz // 2
    narrow = qn.shape[1]

    def ypeer(j):
        return (z, wrap(y + j, ny), t)

    def toff(j):
        core = lax.rem(t, 2)
        return wrap(t - core + 2 * (j // 2), nt) + (core + j % 2 - 2 * core * (j % 2))

    def tpeer(j):
        return (z, y, toff(j))

    far = sorted(range(1, nt), key=lambda j: -min(j // 2, (nt - j) // 2 if j % 2 == 0 else (nt + 1 - j) // 2))

    def rc(src, dst, ssem, rsem, dev):
        return pltpu.make_async_remote_copy(
            src_ref=src, dst_ref=dst, send_sem=ssem, recv_sem=rsem,
            device_id=dev, device_id_type=MESH,
        )

    barrier = pltpu.get_barrier_semaphore()
    peers = [up, dn] + [ypeer(j) for j in range(1, ny)] + [tpeer(j) for j in range(1, nt)]
    for p in peers:
        pl.semaphore_signal(barrier, inc=1, device_id=p, device_id_type=MESH)

    pairs = [
        (kn_in, kv.at[z, 0, pl.ds(0, narrow), :]),
        (vn_in, kv.at[z, 0, pl.ds(narrow, narrow), :]),
        (kb_in, kv.at[z, 1]),
        (vb_in, kv.at[z, 2]),
        (off_in, off.at[z]),
        (qn_in, qs.at[y, pl.ds(0, narrow), :]),
        (qb_in, qs.at[y, pl.ds(narrow, rows), :]),
        (gate_in, w.at[z, y, pl.ds(0, wrows), :]),
        (up_in, w.at[z, y, pl.ds(wrows, wrows), :]),
        (down_in, w.at[z, y, pl.ds(2 * wrows, wrows), :]),
        (on_in, ow.at[t, pl.ds(0, narrow), :]),
        (ob_in, ow.at[t, pl.ds(narrow, rows), :]),
        (stream_in, st),
        (gain_in, gain),
    ]
    copies = [pltpu.make_async_copy(a, b, lsem.at[i]) for i, (a, b) in enumerate(pairs)]
    first, second, third = copies[:10], copies[10:12], copies[12:]
    for c in copies:
        c.start()

    for c in first:
        c.wait()
    pl.semaphore_wait(barrier, len(peers))

    def shard_z(d, k):
        return wrap(z - k, nz) if d == 0 else wrap(z + k, nz)

    def ring(ref, ssem, rsem, d):
        return rc(ref, ref, ssem, rsem, up if d == 0 else dn)

    def kv_ring(d, k, c):
        return ring(kv.at[shard_z(d, k - 1), c], kvs.at[d, k, c], kvr.at[d, k, c], d)

    def off_ring(d, k):
        return ring(off.at[shard_z(d, k - 1)], offs.at[d, k], offr.at[d, k], d)

    def w_ring(d, k):
        return ring(w.at[shard_z(d, k - 1), y], ws.at[d, k], wr.at[d, k], d)

    def w_y(d, k, e):
        ref = w.at[shard_z(d, k), y]
        return rc(ref, ref, yas.at[d, k, e], yar.at[d, k, e], yp if e == 0 else ym)

    def w_relay(d, k):
        src_y = wrap(y - 1, ny) if d == 0 else wrap(y + 1, ny)
        ref = w.at[shard_z(d, k), src_y]
        return rc(ref, ref, yrs.at[d, k], yrr.at[d, k], yp if d == 0 else ym)

    def q_send(j):
        return rc(qs.at[y], qs.at[y], q_s.at[j], q_r.at[j], ypeer(j))

    partner = toff(1)
    xp, xm, xo = toff(2), toff(nt - 2), toff(nt // 2)
    core = lax.rem(t, 2)
    nx = nt // 2

    def ow_send(i):
        src, dst = (
            (t, partner), (t, xp), (t, xm),
            (xm, partner), (xp, partner),
            (jnp.where(core == 0, xm, xp), jnp.where(core == 0, xp, xm)),
            (xo, partner),
        )[i]
        return rc(ow.at[src], ow.at[src], ows.at[i], owr.at[i], (z, y, dst))

    def t_send(g, j):
        ref = tall.at[y, g]
        return rc(ref, ref, t_s.at[g, j], t_r.at[g, j], ypeer(j))

    for j in range(1, ny):
        q_send(j).start()
    for d in range(2):
        off_ring(d, 1).start()
    for c in range(3):
        for d in range(2):
            kv_ring(d, 1, c).start()
    for d in range(2):
        w_ring(d, 1).start()
    for e in range(2):
        w_y(0, 0, e).start()
    for c in second:
        c.wait()
    if nx > 2:
        ow_send(1).start()
        ow_send(2).start()
    ow_send(0).start()

    tcol[...] = jnp.zeros(tcol.shape, F32)

    def zero_body(i, carry):
        obuf[i] = jnp.zeros(obuf.shape[1:], F32)
        return carry

    lax.fori_loop(0, nz + 1, zero_body, 0)
    nq = ny * rows
    key_row = lax.broadcasted_iota(jnp.int32, (2 * rows, 2 * rows), 0)
    key_col = lax.broadcasted_iota(jnp.int32, (2 * rows, 2 * rows), 1)
    same_block = lax.div(key_row, rows) == lax.div(key_col, rows)
    tri = jnp.where(jnp.logical_and(key_row > key_col, same_block), 1.0, 0.0).astype(BF16)
    pick_row = lax.broadcasted_iota(jnp.int32, (2 * rows, 128), 0)
    pick_col = lax.broadcasted_iota(jnp.int32, (2 * rows, 128), 1)

    def totals(blocks, h, diag):
        nk = len(blocks) * rows
        if h == 0:
            keys = [kv[zz, 0, 0:narrow, :] for zz, _, _ in blocks]
            logits = dot(qn[...], jnp.concatenate(keys, axis=1))
        else:
            keys = [kv[zz, 1] for zz, _, _ in blocks]
            logits = dot(qs[:, narrow:, :].reshape(nq, 128), jnp.concatenate(keys, axis=0), NT)
        bias = [off[zz, h : h + 1, :] * LOG2E for zz, _, _ in blocks]
        if not diag:
            bias = [jnp.where(b[2], v, -1e30) for b, v in zip(blocks, bias)]
        logits = logits * SCALE[h] + jnp.concatenate(bias, axis=1)
        soft = jnp.maximum(jnp.log2(1.0 + jnp.exp2(jnp.minimum(logits, 126.0))), logits)
        if diag:
            q_pos = lax.broadcasted_iota(jnp.int32, (nq, rows), 0)
            k_pos = y * rows + lax.broadcasted_iota(jnp.int32, (nq, rows), 1)
            causal = k_pos < q_pos
            low = jnp.where(causal, soft, 0.0).astype(BF16)
        else:
            low = soft.astype(BF16)
        place = 2 * blocks[0][1] + h
        if len(blocks) > 1:
            place = jnp.where(pick_row < rows, place, 2 * blocks[1][1] + h)
        pick = jnp.where(pick_col == place, 1.0, 0.0).astype(BF16)
        tcol[...] += dot(low, pick[0:nk])
        rest = logits - soft
        if diag:
            rest = jnp.where(causal, rest, -1e30)
        lowb[h, :, 0:nk] = low
        gap[h, :, 0:nk] = rest

    def outputs(blocks, h):
        nk = len(blocks) * rows
        weight = jnp.exp2(gap[h, :, 0:nk] - dot(lowb[h, :, 0:nk], tri[0:nk, 0:nk]))
        weight = weight.astype(BF16)
        base = h * narrow
        for i, (zz, s, _) in enumerate(blocks):
            vt = kv[zz, 0, narrow:, :] if h == 0 else jnp.transpose(kv[zz, 2])
            obuf[s, base : base + vt.shape[0], :] = dot(
                vt, weight[:, i * rows : (i + 1) * rows], NT
            )

    def pass_on(make, k):
        for d in range(2):
            def one(d=d):
                make(d, k).wait_recv()

                @pl.when(k < half - d)
                def _():
                    make(d, k + 1).start()

            if d == 0:
                one()
            else:
                pl.when(k < half)(one)

    def forward(k):
        pass_on(off_ring, k)
        for c in range(3):
            pass_on(lambda d, kk, c=c: kv_ring(d, kk, c), k)

    def w_sides(k):
        for e in range(2):
            w_y(0, k, e).start()

        @pl.when(k < half)
        def _():
            for e in range(2):
                w_y(1, k, e).start()

    def relay(d, k):
        w_y(d, k, d).wait_recv()
        w_relay(d, k).start()

    def forward_body(k, carry):
        forward(k)
        return carry

    lax.fori_loop(1, 3, forward_body, 0)
    pass_on(w_ring, jnp.int32(1))
    w_sides(jnp.int32(1))
    w_y(0, 0, 1).wait_recv()
    w_relay(1, 0).start()
    for j in range(1, ny):
        q_send(j).wait_recv()
    for i in range(ny):
        head = jnp.transpose(qs[i, 0:narrow, :].astype(F32))
        qn[i * rows : (i + 1) * rows, :] = head.astype(BF16)
    for h in range(2):
        totals([(z, jnp.int32(0), None)], h, True)
    for h in range(2):
        outputs([(z, jnp.int32(0), None)], h)

    def kv_step(k, carry):
        pl.when(k >= 3)(functools.partial(forward, k))
        blocks = [
            (wrap(z - k, nz), 2 * k - 1, k <= z),
            (wrap(z + k, nz), 2 * k, jnp.logical_and(k < half, z + k >= nz)),
        ]

        def both_totals():
            totals(blocks, 0, False)
            totals(blocks, 1, False)

        def both_outputs():
            outputs(blocks, 0)
            outputs(blocks, 1)

        pl.when(k <= z)(both_totals)

        @pl.when(lax.rem(k, 2) == 0)
        def _():
            g = lax.div(k, 2) - 1
            trow[...] = jnp.transpose(tcol[...])
            tall[y, g] = trow[pl.ds(pl.multiple_of(8 * g, 8), 8), :]
            for j in range(1, ny):
                t_send(g, j).start()

        @pl.when(k >= 3)
        def _():
            pass_on(w_ring, k - 1)
            pl.when(k < half)(functools.partial(w_sides, k - 1))

        @pl.when(jnp.logical_and(k > 3, k < half - 1))
        def _():
            relay(0, k - 3)
            relay(1, k - 3)

        if nx > 2:
            @pl.when(k == half - 2)
            def _():
                ow_send(1).wait_recv()
                ow_send(2).wait_recv()
                ow_send(5).start()
                ow_send(3).start()
                ow_send(4).start()

        pl.when(k <= z)(both_outputs)
        return carry

    lax.fori_loop(1, half + 1, kv_step, 0)

    ngroup = nz // 4
    for g in range(ngroup):
        for j in range(1, ny):
            t_send(g, j).wait_recv()

    trows = ny * ngroup * 8
    nrow = 2 * nz
    flat = tall[...].reshape(trows, nq)
    fr = lax.broadcasted_iota(jnp.int32, (nrow, trows), 0)
    fc = lax.broadcasted_iota(jnp.int32, (nrow, trows), 1)

    def slot_z(slot):
        k = lax.shift_right_logical(slot + 1, 1)
        signed = jnp.where(lax.bitwise_and(slot, 1) == 1, -k, k)
        return lax.bitwise_and(z + signed + nz, nz - 1)

    per_y = ngroup * 8
    c_y = lax.div(fc, per_y)
    c_in = lax.rem(fc, per_y)
    r_order = slot_z(lax.shift_right_logical(fr, 1)) * ny + y
    c_order = slot_z(lax.shift_right_logical(c_in, 1)) * ny + c_y
    same = lax.bitwise_and(fr, 1) == lax.bitwise_and(c_in, 1)
    sel = jnp.where(jnp.logical_and(same, c_order > r_order), 1.0, 0.0).astype(F32)
    later = dot(sel, flat, NN, lax.Precision.HIGHEST)
    fac[...] = jnp.exp2(-later)

    def a_send(j):
        peer = wrap(y + j, ny)
        return rc(ao.at[peer], ar.at[j], a_s.at[j], a_r.at[j], ypeer(j))

    for j in (2, 1, 3, 0) if ny > 2 else range(ny - 1, -1, -1):
        rb = wrap(y + j, ny)
        cols = pl.ds(pl.multiple_of(rb * rows, rows), rows)
        for lo, hi, h in ((0, narrow, 0), (narrow, narrow + 128, 1)):
            part = jnp.zeros((hi - lo, rows), F32)
            for s in range(nz):
                part = part + fac[2 * s + h : 2 * s + h + 1, cols] * obuf[s, lo:hi, cols]
            ao[rb, lo:hi, :] = part.astype(BF16)
        if j > 0:
            a_send(j).start()
    pass_on(w_ring, jnp.int32(half))
    w_sides(jnp.int32(half - 1))
    w_sides(jnp.int32(half))
    early = max(half - 4, 1)
    for k in range(early, half - 1):
        relay(0, k)
        if k >= 1:
            relay(1, k)
    if nx > 2:
        ow_send(5).wait_recv()
        ow_send(6).start()
    attended = ao[y].astype(F32)
    for j in range(1, ny):
        a_send(j).wait_recv()
        attended = attended + ar[j].astype(F32)
    att[t] = attended.astype(BF16)

    def n_send(j):
        return rc(att.at[t], att.at[t], n_s.at[j], n_r.at[j], tpeer(j))

    for j in far:
        n_send(j).start()
    relay(0, half - 1)
    relay(1, half - 1)
    relay(0, half)
    for c in third:
        c.wait()
    if nx > 2:
        for i in (3, 4, 6):
            ow_send(i).wait_recv()
    model = out.shape[1]

    def project(i, head, first):
        for c in range(model // 512):
            cols = slice(c * 512, (c + 1) * 512)
            base = st[:, cols].astype(F32) if first else acc[:, cols]
            acc[:, cols] = base + dot(head, ow[i, :, cols])

    project(t, jnp.transpose(att[t]), True)
    for j in sorted(range(1, nt), key=lambda j: (min(j // 2, nt // 2 - j // 2), j)):
        n_send(j).wait_recv()
        if j == 1:
            ow_send(0).wait_recv()
        i = toff(2 * ((nt // 2 - j // 2) % (nt // 2)) + j % 2)
        project(i, jnp.transpose(att[i]), False)
    square = jnp.zeros((rows, 1), F32)
    for c in range(model // 512):
        cols = slice(c * 512, (c + 1) * 512)
        block = acc[:, cols].astype(BF16)
        st[:, cols] = block
        wide = block.astype(F32)
        square = square + jnp.sum(wide * wide, axis=1, keepdims=True)
    inverse = lax.rsqrt(square * (1.0 / model) + norm_eps)
    for c in range(model // 512):
        cols = slice(c * 512, (c + 1) * 512)
        nb[:, cols] = (st[:, cols].astype(F32) * inverse * gain[:, cols]).astype(BF16)

    w_y(0, 0, 0).wait_recv()
    w_relay(1, 0).wait_recv()

    def w_wait(k, d):
        if d == 0:
            w_y(0, k, 1).wait_recv()
            w_relay(0, k).wait_recv()
        else:
            w_y(1, k, 0).wait_recv()
            w_relay(1, k).wait_recv()

    def w_wait_body(k, carry):
        w_wait(k, 0)

        @pl.when(k < half)
        def _():
            w_wait(k, 1)

        return carry

    lax.fori_loop(1, half + 1, w_wait_body, 0)
    gate = jnp.zeros((rows, w.shape[3]), F32)
    upv = jnp.zeros((rows, w.shape[3]), F32)
    span = ny * wrows
    for zz in range(nz):
        lhs = nb[:, zz * span : (zz + 1) * span]
        gate = gate + dot(lhs, w[zz, :, 0:wrows, :].reshape(span, w.shape[3]))
        upv = upv + dot(lhs, w[zz, :, wrows : 2 * wrows, :].reshape(span, w.shape[3]))
    hidden = (gate / (1.0 + jnp.exp(-gate)) * upv).astype(BF16)
    def r2_send(hf, j):
        return rc(
            part2.at[hf, toff(j)], rs2.at[hf, j], r2s.at[hf, j], r2r.at[hf, j], tpeer(j)
        )

    for hf in range(2):
        for i in range(nz // 2):
            zz = hf * (nz // 2) + i
            rhs = w[zz, :, 2 * wrows :, :].reshape(span, w.shape[3])
            block = dot(hidden, rhs, NT).astype(BF16)
            part2[hf, :, :, i * span : (i + 1) * span] = block.reshape(nt, share, span)
        for j in far:
            r2_send(hf, j).start()

    def drain(k, carry):
        for d in range(2):
            @pl.when(k <= half - d)
            def _():
                for c in range(3):
                    kv_ring(d, k, c).wait_send()
                off_ring(d, k).wait_send()
                w_ring(d, k).wait_send()
                for e in range(2):
                    w_y(d, k, e).wait_send()
                w_relay(d, k).wait_send()
        return carry

    lax.fori_loop(1, half + 1, drain, 0)
    for e in range(2):
        w_y(0, 0, e).wait_send()
    w_relay(1, 0).wait_send()
    for j in range(1, ny):
        q_send(j).wait_send()
        a_send(j).wait_send()
        for g in range(ngroup):
            t_send(g, j).wait_send()
    for j in range(1, nt):
        n_send(j).wait_send()
    ow_send(0).wait_send()
    if nx > 2:
        for i in range(1, 7):
            ow_send(i).wait_send()
    mine = pl.ds(pl.multiple_of(t * share, share), share)
    for hf in range(2):
        cols = slice(hf * model // 2, (hf + 1) * model // 2)
        total = st[mine, cols].astype(F32) + part2[hf, t].astype(F32)
        for j in range(1, nt):
            r2_send(hf, j).wait_recv()
            total = total + rs2[hf, j].astype(F32)
        out[:, cols] = total.astype(BF16)
    for hf in range(2):
        for j in range(1, nt):
            r2_send(hf, j).wait_send()


def local(
    nz, ny, nt,
    stream, query_narrow, query_broad, key_narrow, key_broad, value_narrow, value_broad,
    key_offsets, out_narrow, out_broad, norm_gain, gate_weight, up_weight, down_weight,
):
    rows, model = stream.shape
    wrows, ff = gate_weight.shape
    share = rows // nt
    half = nz // 2
    ngroup = nz // 4
    gain = norm_gain.reshape(1, model)
    dma = pltpu.SemaphoreType.DMA
    scratch = [
        pltpu.VMEM((nz, 3, rows, 128), BF16),
        pltpu.VMEM((nz, 2, rows), F32),
        pltpu.VMEM((ny, 192, 128), BF16),
        pltpu.VMEM((nz, ny, 3 * wrows, ff), BF16),
        pltpu.VMEM((nt, 192, model), BF16),
        pltpu.VMEM((rows, model), BF16),
        pltpu.VMEM((1, model), F32),
        pltpu.VMEM((nz + 1, 192, ny * rows), F32),
        pltpu.VMEM((ny, ngroup, 8, ny * rows), F32),
        pltpu.VMEM((ny, 192, rows), BF16),
        pltpu.VMEM((ny, 192, rows), BF16),
        pltpu.VMEM((nt, 192, rows), BF16),
        pltpu.VMEM((rows, model), BF16),
        pltpu.VMEM((2, nt, share, model // 2), BF16),
        pltpu.VMEM((2, nt, share, model // 2), BF16),
        pltpu.VMEM((ny * rows, 64), BF16),
        pltpu.VMEM((ny * rows, 128), F32),
        pltpu.VMEM((128, ny * rows), F32),
        pltpu.VMEM((2 * nz, ny * rows), F32),
        pltpu.VMEM((rows, model), F32),
        pltpu.VMEM((2, ny * rows, 2 * rows), BF16),
        pltpu.VMEM((2, ny * rows, 2 * rows), F32),
        dma((14,)),
        dma((2, half + 1, 3)), dma((2, half + 1, 3)),
        dma((2, half + 1)), dma((2, half + 1)),
        dma((2, half + 1)), dma((2, half + 1)),
        dma((ny,)), dma((ny,)),
        dma((2, half + 1, 2)), dma((2, half + 1, 2)),
        dma((2, half + 1)), dma((2, half + 1)),
        dma((ngroup, ny)), dma((ngroup, ny)),
        dma((ny,)), dma((ny,)),
        dma((7,)), dma((7,)),
        dma((nt,)), dma((nt,)),
        dma((2, nt)), dma((2, nt)),
    ]
    return pl.pallas_call(
        functools.partial(layer_kernel, nz, ny, nt, rows, wrows, share),
        out_shape=jax.ShapeDtypeStruct((share, model), BF16),
        in_specs=[pl.BlockSpec(memory_space=pl.ANY)] * 14,
        out_specs=pl.BlockSpec(memory_space=pltpu.VMEM),
        scratch_shapes=scratch,
        compiler_params=pltpu.CompilerParams(
            collective_id=0, has_side_effects=True, vmem_limit_bytes=60 * 1024 * 1024
        ),
        name="layer",
    )(
        stream, query_narrow.T, query_broad, key_narrow.T, key_broad, value_narrow.T, value_broad,
        key_offsets.T, out_narrow, out_broad, gain, gate_weight, up_weight, down_weight.T,
    )


def build(mesh, nz, ny, nt):
    torus = Mesh(mesh.devices.reshape(nz, ny, nt), SP_TP)
    in_specs = (
        P(SP, None),
        P(SP, "tp"),
        P(SP, "tp"),
        P(SP, "tp"),
        P(SP, "tp"),
        P(SP, "tp"),
        P(SP, "tp"),
        P(SP, "tp"),
        P("tp", None),
        P("tp", None),
        P(),
        P(SP, "tp"),
        P(SP, "tp"),
        P("tp", SP),
    )
    return jax.shard_map(
        functools.partial(local, nz, ny, nt),
        mesh=torus,
        in_specs=in_specs,
        out_specs=P(SP_TP, None),
        check_vma=False,
    )


def solution(mesh):
    sp = mesh.shape["sp"]
    ny = 4
    return build(mesh, sp // ny, ny, mesh.shape["tp"])
```

```python
import functools
import math

import jax
import jax.numpy as jnp
from jax import lax
from jax.experimental import pallas as pl
from jax.experimental.pallas import tpu as pltpu
from jax.sharding import Mesh
from jax.sharding import PartitionSpec as P

NARROW_SIZE = 64
BROAD_SIZE = 128
SP = ("sp_0", "sp_1")
SP_TP = ("sp_0", "sp_1", "tp")
MESH = pl.DeviceIdType.MESH
LOG2E = 1.4426950408889634
SCALE = (NARROW_SIZE**-0.5 * LOG2E, BROAD_SIZE**-0.5 * LOG2E)
norm_eps = 1e-06
F32 = jnp.float32
BF16 = jnp.bfloat16
NT = (((1,), (1,)), ((), ()))
NN = (((1,), (0,)), ((), ()))


def dot(a, b, dims=NN, precision=None):
    return lax.dot_general(a, b, dims, preferred_element_type=F32, precision=precision)


def wrap(value, size):
    return lax.rem(value + 2 * size, size)


def layer_kernel(
    nz, ny, nt, rows, wrows, share,
    stream_in, qn_in, qb_in, kn_in, kb_in, vn_in, vb_in, off_in, on_in, ob_in, gain_in,
    gate_in, up_in, down_in,
    out,
    kv, off, qs, w, ow, st, gain, obuf, tall, ar, ao, att, nb, part2, rs2,
    qn, tcol, trow, fac, acc, lowb, gap,
    lsem, kvs, kvr, offs, offr, ws, wr, q_s, q_r, yas, yar, yrs, yrr,
    t_s, t_r, a_s, a_r, ows, owr, n_s, n_r, r2s, r2r,
):
    z = lax.axis_index("sp_0")
    y = lax.axis_index("sp_1")
    t = lax.axis_index("tp")
    up = (wrap(z + 1, nz), y, t)
    dn = (wrap(z - 1, nz), y, t)
    yp = (z, wrap(y + 1, ny), t)
    ym = (z, wrap(y - 1, ny), t)
    half = nz // 2
    narrow = qn.shape[1]

    def ypeer(j):
        return (z, wrap(y + j, ny), t)

    def toff(j):
        core = lax.rem(t, 2)
        return wrap(t - core + 2 * (j // 2), nt) + (core + j % 2 - 2 * core * (j % 2))

    def tpeer(j):
        return (z, y, toff(j))

    far = sorted(range(1, nt), key=lambda j: -min(j // 2, (nt - j) // 2 if j % 2 == 0 else (nt + 1 - j) // 2))

    def rc(src, dst, ssem, rsem, dev):
        return pltpu.make_async_remote_copy(
            src_ref=src, dst_ref=dst, send_sem=ssem, recv_sem=rsem,
            device_id=dev, device_id_type=MESH,
        )

    barrier = pltpu.get_barrier_semaphore()
    peers = [up, dn] + [ypeer(j) for j in range(1, ny)] + [tpeer(j) for j in range(1, nt)]
    for p in peers:
        pl.semaphore_signal(barrier, inc=1, device_id=p, device_id_type=MESH)

    pairs = [
        (kn_in, kv.at[z, 0, pl.ds(0, narrow), :]),
        (vn_in, kv.at[z, 0, pl.ds(narrow, narrow), :]),
        (kb_in, kv.at[z, 1]),
        (vb_in, kv.at[z, 2]),
        (off_in, off.at[z]),
        (qn_in, qs.at[y, pl.ds(0, narrow), :]),
        (qb_in, qs.at[y, pl.ds(narrow, rows), :]),
        (gate_in, w.at[z, y, pl.ds(0, wrows), :]),
        (up_in, w.at[z, y, pl.ds(wrows, wrows), :]),
        (down_in, w.at[z, y, pl.ds(2 * wrows, wrows), :]),
        (on_in, ow.at[t, pl.ds(0, narrow), :]),
        (ob_in, ow.at[t, pl.ds(narrow, rows), :]),
        (stream_in, st),
        (gain_in, gain),
    ]
    copies = [pltpu.make_async_copy(a, b, lsem.at[i]) for i, (a, b) in enumerate(pairs)]
    first, second, third = copies[:10], copies[10:12], copies[12:]
    for c in copies:
        c.start()

    for c in first:
        c.wait()
    pl.semaphore_wait(barrier, len(peers))

    def shard_z(d, k):
        return wrap(z - k, nz) if d == 0 else wrap(z + k, nz)

    def ring(ref, ssem, rsem, d):
        return rc(ref, ref, ssem, rsem, up if d == 0 else dn)

    def kv_ring(d, k, c):
        return ring(kv.at[shard_z(d, k - 1), c], kvs.at[d, k, c], kvr.at[d, k, c], d)

    def off_ring(d, k):
        return ring(off.at[shard_z(d, k - 1)], offs.at[d, k], offr.at[d, k], d)

    def w_ring(d, k):
        return ring(w.at[shard_z(d, k - 1), y], ws.at[d, k], wr.at[d, k], d)

    def w_y(d, k, e):
        ref = w.at[shard_z(d, k), y]
        return rc(ref, ref, yas.at[d, k, e], yar.at[d, k, e], yp if e == 0 else ym)

    def w_relay(d, k):
        src_y = wrap(y - 1, ny) if d == 0 else wrap(y + 1, ny)
        ref = w.at[shard_z(d, k), src_y]
        return rc(ref, ref, yrs.at[d, k], yrr.at[d, k], yp if d == 0 else ym)

    def q_send(j):
        return rc(qs.at[y], qs.at[y], q_s.at[j], q_r.at[j], ypeer(j))

    partner = toff(1)
    xp, xm, xo = toff(2), toff(nt - 2), toff(nt // 2)
    core = lax.rem(t, 2)
    nx = nt // 2

    def ow_send(i):
        src, dst = (
            (t, partner), (t, xp), (t, xm),
            (xm, partner), (xp, partner),
            (jnp.where(core == 0, xm, xp), jnp.where(core == 0, xp, xm)),
            (xo, partner),
        )[i]
        return rc(ow.at[src], ow.at[src], ows.at[i], owr.at[i], (z, y, dst))

    def t_send(g, j):
        ref = tall.at[y, g]
        return rc(ref, ref, t_s.at[g, j], t_r.at[g, j], ypeer(j))

    for j in range(1, ny):
        q_send(j).start()
    for d in range(2):
        off_ring(d, 1).start()
    for c in range(3):
        for d in range(2):
            kv_ring(d, 1, c).start()
    for d in range(2):
        w_ring(d, 1).start()
    for e in range(2):
        w_y(0, 0, e).start()
    for c in second:
        c.wait()
    if nx > 2:
        ow_send(1).start()
        ow_send(2).start()
    ow_send(0).start()

    tcol[...] = jnp.zeros(tcol.shape, F32)

    def zero_body(i, carry):
        obuf[i] = jnp.zeros(obuf.shape[1:], F32)
        return carry

    lax.fori_loop(0, nz + 1, zero_body, 0)
    nq = ny * rows
    key_row = lax.broadcasted_iota(jnp.int32, (2 * rows, 2 * rows), 0)
    key_col = lax.broadcasted_iota(jnp.int32, (2 * rows, 2 * rows), 1)
    same_block = lax.div(key_row, rows) == lax.div(key_col, rows)
    tri = jnp.where(jnp.logical_and(key_row > key_col, same_block), 1.0, 0.0).astype(BF16)
    pick_row = lax.broadcasted_iota(jnp.int32, (2 * rows, 128), 0)
    pick_col = lax.broadcasted_iota(jnp.int32, (2 * rows, 128), 1)

    def totals(blocks, h, diag):
        nk = len(blocks) * rows
        if h == 0:
            keys = [kv[zz, 0, 0:narrow, :] for zz, _, _ in blocks]
            logits = dot(qn[...], jnp.concatenate(keys, axis=1))
        else:
            keys = [kv[zz, 1] for zz, _, _ in blocks]
            logits = dot(qs[:, narrow:, :].reshape(nq, 128), jnp.concatenate(keys, axis=0), NT)
        bias = [off[zz, h : h + 1, :] * LOG2E for zz, _, _ in blocks]
        if not diag:
            bias = [jnp.where(b[2], v, -1e30) for b, v in zip(blocks, bias)]
        logits = logits * SCALE[h] + jnp.concatenate(bias, axis=1)
        soft = jnp.maximum(jnp.log2(1.0 + jnp.exp2(jnp.minimum(logits, 126.0))), logits)
        if diag:
            q_pos = lax.broadcasted_iota(jnp.int32, (nq, rows), 0)
            k_pos = y * rows + lax.broadcasted_iota(jnp.int32, (nq, rows), 1)
            causal = k_pos < q_pos
            low = jnp.where(causal, soft, 0.0).astype(BF16)
        else:
            low = soft.astype(BF16)
        place = 2 * blocks[0][1] + h
        if len(blocks) > 1:
            place = jnp.where(pick_row < rows, place, 2 * blocks[1][1] + h)
        pick = jnp.where(pick_col == place, 1.0, 0.0).astype(BF16)
        tcol[...] += dot(low, pick[0:nk])
        rest = logits - soft
        if diag:
            rest = jnp.where(causal, rest, -1e30)
        lowb[h, :, 0:nk] = low
        gap[h, :, 0:nk] = rest

    def outputs(blocks, h):
        nk = len(blocks) * rows
        weight = jnp.exp2(gap[h, :, 0:nk] - dot(lowb[h, :, 0:nk], tri[0:nk, 0:nk]))
        weight = weight.astype(BF16)
        base = h * narrow
        for i, (zz, s, _) in enumerate(blocks):
            vt = kv[zz, 0, narrow:, :] if h == 0 else jnp.transpose(kv[zz, 2])
            obuf[s, base : base + vt.shape[0], :] = dot(
                vt, weight[:, i * rows : (i + 1) * rows], NT
            )

    def pass_on(make, k):
        for d in range(2):
            def one(d=d):
                make(d, k).wait_recv()

                @pl.when(k < half - d)
                def _():
                    make(d, k + 1).start()

            if d == 0:
                one()
            else:
                pl.when(k < half)(one)

    def forward(k):
        pass_on(off_ring, k)
        for c in range(3):
            pass_on(lambda d, kk, c=c: kv_ring(d, kk, c), k)

    def w_sides(k):
        for e in range(2):
            w_y(0, k, e).start()

        @pl.when(k < half)
        def _():
            for e in range(2):
                w_y(1, k, e).start()

    def relay(d, k):
        w_y(d, k, d).wait_recv()
        w_relay(d, k).start()

    forward(jnp.int32(1))
    pass_on(w_ring, jnp.int32(1))
    w_sides(jnp.int32(1))
    w_y(0, 0, 1).wait_recv()
    w_relay(1, 0).start()
    forward(jnp.int32(2))
    for j in range(1, ny):
        q_send(j).wait_recv()
    for i in range(ny):
        head = jnp.transpose(qs[i, 0:narrow, :].astype(F32))
        qn[i * rows : (i + 1) * rows, :] = head.astype(BF16)
    for h in range(2):
        totals([(z, jnp.int32(0), None)], h, True)
    for h in range(2):
        outputs([(z, jnp.int32(0), None)], h)

    def kv_step(k, carry):
        pl.when(k >= 3)(functools.partial(forward, k))
        blocks = [
            (wrap(z - k, nz), 2 * k - 1, k <= z),
            (wrap(z + k, nz), 2 * k, jnp.logical_and(k < half, z + k >= nz)),
        ]

        def both_totals():
            totals(blocks, 0, False)
            totals(blocks, 1, False)

        def both_outputs():
            outputs(blocks, 0)
            outputs(blocks, 1)

        pl.when(k <= z)(both_totals)

        @pl.when(lax.rem(k, 2) == 0)
        def _():
            g = lax.div(k, 2) - 1
            trow[...] = jnp.transpose(tcol[...])
            tall[y, g] = trow[pl.ds(pl.multiple_of(8 * g, 8), 8), :]
            for j in range(1, ny):
                t_send(g, j).start()

        @pl.when(jnp.logical_and(k >= 2, k < half))
        def _():
            pass_on(w_ring, k)
            w_sides(k)

        @pl.when(jnp.logical_and(k > 3, k < half - 2))
        def _():
            relay(0, k - 3)
            relay(1, k - 3)

        if nx > 2:
            @pl.when(k == half - 2)
            def _():
                ow_send(1).wait_recv()
                ow_send(2).wait_recv()
                ow_send(5).start()
                ow_send(3).start()
                ow_send(4).start()

        pl.when(k <= z)(both_outputs)
        return carry

    lax.fori_loop(1, half + 1, kv_step, 0)

    ngroup = nz // 4
    for g in range(ngroup):
        for j in range(1, ny):
            t_send(g, j).wait_recv()

    trows = ny * ngroup * 8
    nrow = 2 * nz
    flat = tall[...].reshape(trows, nq)
    fr = lax.broadcasted_iota(jnp.int32, (nrow, trows), 0)
    fc = lax.broadcasted_iota(jnp.int32, (nrow, trows), 1)

    def slot_z(slot):
        k = lax.shift_right_logical(slot + 1, 1)
        signed = jnp.where(lax.bitwise_and(slot, 1) == 1, -k, k)
        return lax.bitwise_and(z + signed + nz, nz - 1)

    per_y = ngroup * 8
    c_y = lax.div(fc, per_y)
    c_in = lax.rem(fc, per_y)
    r_order = slot_z(lax.shift_right_logical(fr, 1)) * ny + y
    c_order = slot_z(lax.shift_right_logical(c_in, 1)) * ny + c_y
    same = lax.bitwise_and(fr, 1) == lax.bitwise_and(c_in, 1)
    sel = jnp.where(jnp.logical_and(same, c_order > r_order), 1.0, 0.0).astype(F32)
    later = dot(sel, flat, NN, lax.Precision.HIGHEST)
    fac[...] = jnp.exp2(-later)

    def a_send(j):
        peer = wrap(y + j, ny)
        return rc(ao.at[peer], ar.at[j], a_s.at[j], a_r.at[j], ypeer(j))

    for j in (2, 1, 3, 0) if ny > 2 else range(ny - 1, -1, -1):
        rb = wrap(y + j, ny)
        cols = pl.ds(pl.multiple_of(rb * rows, rows), rows)
        for lo, hi, h in ((0, narrow, 0), (narrow, narrow + 128, 1)):
            part = jnp.zeros((hi - lo, rows), F32)
            for s in range(nz):
                part = part + fac[2 * s + h : 2 * s + h + 1, cols] * obuf[s, lo:hi, cols]
            ao[rb, lo:hi, :] = part.astype(BF16)
        if j > 0:
            a_send(j).start()
    pass_on(w_ring, jnp.int32(half))
    w_sides(jnp.int32(half))
    early = max(half - 5, 1)
    for k in range(early, half - 1):
        relay(0, k)
        if k >= 1:
            relay(1, k)
    if nx > 2:
        ow_send(5).wait_recv()
        ow_send(6).start()
    attended = ao[y].astype(F32)
    for j in range(1, ny):
        a_send(j).wait_recv()
        attended = attended + ar[j].astype(F32)
    att[t] = attended.astype(BF16)

    def n_send(j):
        return rc(att.at[t], att.at[t], n_s.at[j], n_r.at[j], tpeer(j))

    for j in far:
        n_send(j).start()
    relay(0, half - 1)
    relay(1, half - 1)
    relay(0, half)
    for c in third:
        c.wait()
    if nx > 2:
        for i in (3, 4, 6):
            ow_send(i).wait_recv()
    model = out.shape[1]

    def project(i, head, first):
        for c in range(model // 512):
            cols = slice(c * 512, (c + 1) * 512)
            base = st[:, cols].astype(F32) if first else acc[:, cols]
            acc[:, cols] = base + dot(head, ow[i, :, cols])

    project(t, jnp.transpose(att[t]), True)
    for j in sorted(range(1, nt), key=lambda j: (min(j // 2, nt // 2 - j // 2), j)):
        n_send(j).wait_recv()
        if j == 1:
            ow_send(0).wait_recv()
        i = toff(2 * ((nt // 2 - j // 2) % (nt // 2)) + j % 2)
        project(i, jnp.transpose(att[i]), False)
    square = jnp.zeros((rows, 1), F32)
    for c in range(model // 512):
        cols = slice(c * 512, (c + 1) * 512)
        block = acc[:, cols].astype(BF16)
        st[:, cols] = block
        wide = block.astype(F32)
        square = square + jnp.sum(wide * wide, axis=1, keepdims=True)
    inverse = lax.rsqrt(square * (1.0 / model) + norm_eps)
    for c in range(model // 512):
        cols = slice(c * 512, (c + 1) * 512)
        nb[:, cols] = (st[:, cols].astype(F32) * inverse * gain[:, cols]).astype(BF16)

    w_y(0, 0, 0).wait_recv()
    w_relay(1, 0).wait_recv()

    def w_wait(k, d):
        if d == 0:
            w_y(0, k, 1).wait_recv()
            w_relay(0, k).wait_recv()
        else:
            w_y(1, k, 0).wait_recv()
            w_relay(1, k).wait_recv()

    def w_wait_body(k, carry):
        w_wait(k, 0)

        @pl.when(k < half)
        def _():
            w_wait(k, 1)

        return carry

    lax.fori_loop(1, half + 1, w_wait_body, 0)
    gate = jnp.zeros((rows, w.shape[3]), F32)
    upv = jnp.zeros((rows, w.shape[3]), F32)
    span = ny * wrows
    for zz in range(nz):
        lhs = nb[:, zz * span : (zz + 1) * span]
        gate = gate + dot(lhs, w[zz, :, 0:wrows, :].reshape(span, w.shape[3]))
        upv = upv + dot(lhs, w[zz, :, wrows : 2 * wrows, :].reshape(span, w.shape[3]))
    hidden = (gate / (1.0 + jnp.exp(-gate)) * upv).astype(BF16)
    def r2_send(hf, j):
        return rc(
            part2.at[hf, toff(j)], rs2.at[hf, j], r2s.at[hf, j], r2r.at[hf, j], tpeer(j)
        )

    for hf in range(2):
        for i in range(nz // 2):
            zz = hf * (nz // 2) + i
            rhs = w[zz, :, 2 * wrows :, :].reshape(span, w.shape[3])
            block = dot(hidden, rhs, NT).astype(BF16)
            part2[hf, :, :, i * span : (i + 1) * span] = block.reshape(nt, share, span)
        for j in far:
            r2_send(hf, j).start()

    def drain(k, carry):
        for d in range(2):
            @pl.when(k <= half - d)
            def _():
                for c in range(3):
                    kv_ring(d, k, c).wait_send()
                off_ring(d, k).wait_send()
                w_ring(d, k).wait_send()
                for e in range(2):
                    w_y(d, k, e).wait_send()
                w_relay(d, k).wait_send()
        return carry

    lax.fori_loop(1, half + 1, drain, 0)
    for e in range(2):
        w_y(0, 0, e).wait_send()
    w_relay(1, 0).wait_send()
    for j in range(1, ny):
        q_send(j).wait_send()
        a_send(j).wait_send()
        for g in range(ngroup):
            t_send(g, j).wait_send()
    for j in range(1, nt):
        n_send(j).wait_send()
    ow_send(0).wait_send()
    if nx > 2:
        for i in range(1, 7):
            ow_send(i).wait_send()
    mine = pl.ds(pl.multiple_of(t * share, share), share)
    for hf in range(2):
        cols = slice(hf * model // 2, (hf + 1) * model // 2)
        total = st[mine, cols].astype(F32) + part2[hf, t].astype(F32)
        for j in range(1, nt):
            r2_send(hf, j).wait_recv()
            total = total + rs2[hf, j].astype(F32)
        out[:, cols] = total.astype(BF16)
    for hf in range(2):
        for j in range(1, nt):
            r2_send(hf, j).wait_send()


def local(
    nz, ny, nt,
    stream, query_narrow, query_broad, key_narrow, key_broad, value_narrow, value_broad,
    key_offsets, out_narrow, out_broad, norm_gain, gate_weight, up_weight, down_weight,
):
    rows, model = stream.shape
    wrows, ff = gate_weight.shape
    share = rows // nt
    half = nz // 2
    ngroup = nz // 4
    gain = norm_gain.reshape(1, model)
    dma = pltpu.SemaphoreType.DMA
    scratch = [
        pltpu.VMEM((nz, 3, rows, 128), BF16),
        pltpu.VMEM((nz, 2, rows), F32),
        pltpu.VMEM((ny, 192, 128), BF16),
        pltpu.VMEM((nz, ny, 3 * wrows, ff), BF16),
        pltpu.VMEM((nt, 192, model), BF16),
        pltpu.VMEM((rows, model), BF16),
        pltpu.VMEM((1, model), F32),
        pltpu.VMEM((nz + 1, 192, ny * rows), F32),
        pltpu.VMEM((ny, ngroup, 8, ny * rows), F32),
        pltpu.VMEM((ny, 192, rows), BF16),
        pltpu.VMEM((ny, 192, rows), BF16),
        pltpu.VMEM((nt, 192, rows), BF16),
        pltpu.VMEM((rows, model), BF16),
        pltpu.VMEM((2, nt, share, model // 2), BF16),
        pltpu.VMEM((2, nt, share, model // 2), BF16),
        pltpu.VMEM((ny * rows, 64), BF16),
        pltpu.VMEM((ny * rows, 128), F32),
        pltpu.VMEM((128, ny * rows), F32),
        pltpu.VMEM((2 * nz, ny * rows), F32),
        pltpu.VMEM((rows, model), F32),
        pltpu.VMEM((2, ny * rows, 2 * rows), BF16),
        pltpu.VMEM((2, ny * rows, 2 * rows), F32),
        dma((14,)),
        dma((2, half + 1, 3)), dma((2, half + 1, 3)),
        dma((2, half + 1)), dma((2, half + 1)),
        dma((2, half + 1)), dma((2, half + 1)),
        dma((ny,)), dma((ny,)),
        dma((2, half + 1, 2)), dma((2, half + 1, 2)),
        dma((2, half + 1)), dma((2, half + 1)),
        dma((ngroup, ny)), dma((ngroup, ny)),
        dma((ny,)), dma((ny,)),
        dma((7,)), dma((7,)),
        dma((nt,)), dma((nt,)),
        dma((2, nt)), dma((2, nt)),
    ]
    return pl.pallas_call(
        functools.partial(layer_kernel, nz, ny, nt, rows, wrows, share),
        out_shape=jax.ShapeDtypeStruct((share, model), BF16),
        in_specs=[pl.BlockSpec(memory_space=pl.ANY)] * 14,
        out_specs=pl.BlockSpec(memory_space=pltpu.VMEM),
        scratch_shapes=scratch,
        compiler_params=pltpu.CompilerParams(
            collective_id=0, has_side_effects=True, vmem_limit_bytes=60 * 1024 * 1024
        ),
        name="layer",
    )(
        stream, query_narrow.T, query_broad, key_narrow.T, key_broad, value_narrow.T, value_broad,
        key_offsets.T, out_narrow, out_broad, gain, gate_weight, up_weight, down_weight.T,
    )


def build(mesh, nz, ny, nt):
    torus = Mesh(mesh.devices.reshape(nz, ny, nt), SP_TP)
    in_specs = (
        P(SP, None),
        P(SP, "tp"),
        P(SP, "tp"),
        P(SP, "tp"),
        P(SP, "tp"),
        P(SP, "tp"),
        P(SP, "tp"),
        P(SP, "tp"),
        P("tp", None),
        P("tp", None),
        P(),
        P(SP, "tp"),
        P(SP, "tp"),
        P("tp", SP),
    )
    return jax.shard_map(
        functools.partial(local, nz, ny, nt),
        mesh=torus,
        in_specs=in_specs,
        out_specs=P(SP_TP, None),
        check_vma=False,
    )


def solution(mesh):
    sp = mesh.shape["sp"]
    ny = 4
    return build(mesh, sp // ny, ny, mesh.shape["tp"])
```
